32 devices in a mesh: sp: 8 (over z, core), tp: 4 (over y, x).
Axes of the slice: x: 2, y: 2, z: 4, core: 2. Of those that a mesh axis runs over, the one named last changes fastest.
Arguments:
- query_a: bfloat16 [1024, 1024], P('tp', 'sp'), may hold values from -16 to 16
- key_a: bfloat16 [1024, 1024], P('tp', 'sp'), may hold values from -6 to 6
- value_a: bfloat16 [1024, 1024], P('tp', 'sp'), may hold values from -6 to 6
- cumlog_a: float32 [16, 1024], P('tp'), as said below
- query_b: bfloat16 [2048, 1024], P('tp', 'sp'), may hold values from -16 to 16
- key_b: bfloat16 [2048, 1024], P('tp', 'sp'), may hold values from -6 to 6
- value_b: bfloat16 [2048, 1024], P('tp', 'sp'), may hold values from -6 to 6
- cumlog_b: float32 [16, 1024], P('tp'), as said below
- out_weight_a: bfloat16 [1024, 2048], P('tp'), may hold values from -0.375 to 0.375
- out_weight_b: bfloat16 [2048, 2048], P('tp'), may hold values from -0.25 to 0.25
- residual: bfloat16 [1024, 2048], P(('sp', 'tp')), may hold values from -6 to 6
- norm_gain: float32 [2048], replicated, may hold values from 0.1 to 1.9
- expert_ids: int32 [1024, 2], P('sp'), may hold values from 0 to 7, as said below
- route_weight: float32 [1024, 2], P('sp'), may hold values from 0.1 to 1
- gate_w: bfloat16 [8, 2048, 1024], P('sp', None, 'tp'), may hold values from -0.125 to 0.125
- up_w: bfloat16 [8, 2048, 1024], P('sp', None, 'tp'), may hold values from -0.125 to 0.125
- down_w: bfloat16 [8, 1024, 2048], P('sp', None, 'tp'), may hold values from -0.1875 to 0.1875
Outputs:
- layer_out: bfloat16 [1024, 2048], P('sp', 'tp')
The draws below stay inside these ranges and needn't reach their ends.
Inputs may be any that keep to these rules, and one draw needn't show every extreme that they name: `expert_ids`: each row names two different experts of one group (expert e is in group e // 2). In every aligned block of 128 rows (one index of sp) no expert is named more than 64 times, and every expert of one group, the same group for all blocks, is named exactly 64 times. `cumlog_a`: along positions the values of each head never increase. `cumlog_b`: along positions the values of each head never increase.
All inputs are finite; a program needn't handle non-finite values.
Results may differ from the reference program's by a relative error of at most 0.017.
Values may be sent and summed in bfloat16 or wider, within the bound.
A program may use at most 64 MiB of HBM per device.

```python
import jax
import jax.numpy as jnp
from jax import lax

D = 2048
HA = 16
HDA = 64
HB = 16
HDB = 128
DFF = 1024
GROUPS = 4
TOP = 2
TOK_DEV = 128
TOKENS = 1024
EXPERTS = 8
GSZ = 2
CAP = 64
N_SP = 8
N_TP = 4


def query_like(key, rows, salt):
    own = jax.random.fold_in(key, salt)
    base = jnp.clip(2.5 * jax.random.normal(own, (rows, TOKENS), jnp.float32), -15.0, 15.0)
    return base.astype(jnp.bfloat16)


def key_like(key, rows, salt):
    own = jax.random.fold_in(key, salt)
    base = jnp.clip(jax.random.normal(own, (rows, TOKENS), jnp.float32), -6.0, 6.0)
    return base.astype(jnp.bfloat16)


def draw_query_a(key, part):
    return query_like(key, HA * HDA, 1)


def draw_key_a(key, part):
    return key_like(key, HA * HDA, 2)


def draw_query_b(key, part):
    return query_like(key, HB * HDB, 3)


def draw_key_b(key, part):
    return key_like(key, HB * HDB, 4)


def gate_totals(key, heads):
    order = jax.random.permutation(jax.random.fold_in(key, 11), heads)
    slow = order < heads // 2
    rate_slow = 1.5 / TOKENS * jax.random.uniform(jax.random.fold_in(key, 12), (heads,), jnp.float32, 0.5, 1.2)
    rate_fast = jax.random.uniform(jax.random.fold_in(key, 13), (heads,), jnp.float32, 0.01, 0.033)
    rate = jnp.where(slow, rate_slow, rate_fast)
    block_factor = jnp.exp(jax.random.uniform(jax.random.fold_in(key, 14), (heads, TOKENS // TOK_DEV), jnp.float32, -0.9, 0.9))
    factor = jnp.repeat(block_factor, TOK_DEV, axis=1)
    rough = jax.random.uniform(jax.random.fold_in(key, 15), (heads, TOKENS), jnp.float32, 0.3, 1.7)
    return jnp.cumsum(-rate[:, None] * factor * rough, axis=1).astype(jnp.float32)


def draw_cumlog_a(key, part):
    return gate_totals(jax.random.fold_in(key, 5), HA)


def draw_cumlog_b(key, part):
    return gate_totals(jax.random.fold_in(key, 6), HB)


def draw_expert_ids(key, part):
    hot = jax.random.randint(jax.random.fold_in(key, 21), (), 0, GROUPS)

    def one_block(block_index):
        block_key = jax.random.fold_in(key, 1000 + block_index)

        def group_pairs(group):
            perm = jax.random.permutation(jax.random.fold_in(block_key, group), GSZ)
            spots = jnp.arange(TOK_DEV // 2) % GSZ
            return jnp.stack([perm[spots], perm[(spots + 1) % GSZ]], axis=-1) + group * GSZ
        pairs = jax.vmap(group_pairs)(jnp.arange(GROUPS))
        order = jnp.argsort(jnp.where(jnp.arange(GROUPS) == hot, 0, 1), stable=True)
        pairs = pairs[order]
        others = pairs[1:].reshape(-1, 2)
        chosen = jax.random.permutation(jax.random.fold_in(block_key, 50), others.shape[0])[:TOK_DEV // 2]
        rows = jnp.concatenate([pairs[0], others[chosen]], axis=0)
        shuffle = jax.random.permutation(jax.random.fold_in(block_key, 51), TOK_DEV)
        return rows[shuffle]
    blocks = jax.vmap(one_block)(jnp.arange(TOKENS // TOK_DEV))
    return blocks.reshape(TOKENS, TOP).astype(jnp.int32)


def level_of(key, extent, cuts, smallest, high):
    def one(position, blocks):
        steps = jax.random.uniform(jax.random.fold_in(jax.random.fold_in(key, 6), position), (blocks,), jnp.float32, smallest / len(cuts), high / len(cuts))
        return jnp.repeat(jnp.exp(steps), extent[position] // blocks).reshape((-1,) + (1,) * (len(extent) - position - 1))

    loudness = one(*cuts[0])
    for cut in cuts[1:]:
        loudness = loudness * one(*cut)
    return loudness


def gaussian(own_key, dims, deviation, limit, split=(), kind=jnp.bfloat16):
    array = deviation * jax.random.normal(own_key, dims, jnp.float32)
    if split:
        array = array * level_of(own_key, dims, split, -0.22, 0.18)
    return jnp.clip(array, -limit, limit).astype(kind)


def setup_inputs(seed: int = 0) -> dict:
    key_list = jax.random.split(jax.random.key(seed), 18)
    query_a = draw_query_a(jax.random.fold_in(key_list[17], 71), 0)
    key_a = draw_key_a(jax.random.fold_in(key_list[17], 71), 0)
    value_a = gaussian(key_list[2], (HA * HDA, TOKENS), 1.0, 6.0, ((0, 4), (1, 8)))
    cumlog_a = draw_cumlog_a(jax.random.fold_in(key_list[17], 71), 0)
    query_b = draw_query_b(jax.random.fold_in(key_list[17], 71), 0)
    key_b = draw_key_b(jax.random.fold_in(key_list[17], 71), 0)
    value_b = gaussian(key_list[6], (HB * HDB, TOKENS), 1.0, 6.0, ((0, 4), (1, 8)))
    cumlog_b = draw_cumlog_b(jax.random.fold_in(key_list[17], 71), 0)
    out_weight_a = gaussian(key_list[8], (HA * HDA, D), (HA * HDA // 4) ** -0.5, 0.375, ((0, 4),))
    out_weight_b = gaussian(key_list[9], (HB * HDB, D), (HB * HDB // 4) ** -0.5, 0.25, ((0, 4),))
    residual = gaussian(key_list[10], (TOKENS, D), 1.0, 6.0, ((0, 32),))
    norm_gain = jnp.clip(1.0 + 0.18 * jax.random.normal(key_list[11], (D,), jnp.float32), 0.1, 1.9)
    expert_ids = draw_expert_ids(jax.random.fold_in(key_list[17], 71), 0)
    route_weight = jnp.clip(0.1 + 0.9 * jax.random.uniform(key_list[13], (TOKENS, TOP), jnp.float32) ** level_of(key_list[13], (TOKENS, TOP), ((0, 8),), -0.2, 0.2), 0.1, 1.0)
    gate_w = gaussian(key_list[14], (EXPERTS, D, DFF), D ** -0.5, 0.125, ((0, 8), (2, 4)))
    up_w = gaussian(key_list[15], (EXPERTS, D, DFF), D ** -0.5, 0.125, ((0, 8), (2, 4)))
    down_w = gaussian(key_list[16], (EXPERTS, DFF, D), DFF ** -0.5, 0.1875, ((0, 8), (2, 4)))
    return {"query_a": query_a, "key_a": key_a, "value_a": value_a, "cumlog_a": cumlog_a, "query_b": query_b, "key_b": key_b, "value_b": value_b, "cumlog_b": cumlog_b, "out_weight_a": out_weight_a, "out_weight_b": out_weight_b, "residual": residual, "norm_gain": norm_gain, "expert_ids": expert_ids, "route_weight": route_weight, "gate_w": gate_w, "up_w": up_w, "down_w": down_w}


norm_eps = 1e-05

def attend_group(queries, keys_in, values_in, gate_sums, heads, head_size):
    length = queries.shape[1]
    span = 256
    count_blocks = length // span
    query_heads = queries.reshape(heads, head_size, length)
    key_heads = keys_in.reshape(heads, head_size, length).astype(jnp.float32)
    value_heads = values_in.reshape(heads, head_size, length).astype(jnp.float32)
    positions = jnp.arange(length, dtype=jnp.int32)

    def one_block(index):
        offset = (index * span).astype(jnp.int32)
        query_block = lax.dynamic_slice_in_dim(query_heads, offset, span, 2).astype(jnp.float32)
        cum_block = lax.dynamic_slice_in_dim(gate_sums, offset, span, 1)
        scores = jnp.einsum('hdq,hdk->hqk', query_block, key_heads) * head_size ** (-0.5)
        scores = scores + cum_block[:, :, None] - gate_sums[:, None, :]
        rows_at = offset + jnp.arange(span, dtype=jnp.int32)
        scores = jnp.where(positions[None, None, :] <= rows_at[None, :, None], scores, -jnp.inf)
        weights = jax.nn.softmax(scores, axis=-1).astype(jnp.bfloat16)
        return jnp.einsum('hqk,hdk->hdq', weights.astype(jnp.float32), value_heads).astype(jnp.bfloat16)
    blocks = lax.map(one_block, jnp.arange(count_blocks, dtype=jnp.int32))
    return blocks.transpose(1, 2, 0, 3).reshape(heads * head_size, length)

def project_out(attn_a, attn_b, out_weight_a, out_weight_b):
    length = attn_a.shape[1]
    rows_a = attn_a.shape[0] // N_TP
    rows_b = attn_b.shape[0] // N_TP

    def add_part(total, index):
        part_a = lax.dynamic_slice_in_dim(attn_a, index * rows_a, rows_a, 0)
        part_b = lax.dynamic_slice_in_dim(attn_b, index * rows_b, rows_b, 0)
        weight_a = lax.dynamic_slice_in_dim(out_weight_a, index * rows_a, rows_a, 0)
        weight_b = lax.dynamic_slice_in_dim(out_weight_b, index * rows_b, rows_b, 0)
        term = jnp.dot(part_a.T, weight_a, preferred_element_type=jnp.float32)
        term = term + jnp.dot(part_b.T, weight_b, preferred_element_type=jnp.float32)
        rounded = lax.optimization_barrier(term.astype(jnp.bfloat16))
        return (total + rounded.astype(jnp.float32), None)
    total, _ = lax.scan(add_part, jnp.zeros((length, D), jnp.float32), jnp.arange(N_TP, dtype=jnp.int32))
    return total

def experts_out(normed, expert_ids, route_weight, gate_w, up_w, down_w):
    flat_ids = expert_ids.reshape(N_SP, TOK_DEV * TOP)
    marks = (flat_ids[:, :, None] == jnp.arange(EXPERTS, dtype=jnp.int32)[None, None, :]).astype(jnp.int32)
    before = jnp.cumsum(marks, axis=1) - marks
    rank = lax.optimization_barrier(jnp.sum(before * marks, axis=2))
    source = jnp.arange(N_SP, dtype=jnp.int32)[:, None]
    per_expert = N_SP * CAP
    where_to = (flat_ids * per_expert + source * CAP + rank).reshape(-1).astype(jnp.int32)
    token_of = jnp.repeat(jnp.arange(TOKENS, dtype=jnp.int32), TOP)
    table = jnp.zeros((EXPERTS * per_expert,), jnp.int32).at[where_to].set(token_of)
    filled = jnp.zeros((EXPERTS * per_expert,), jnp.float32).at[where_to].set(1.0)

    def one_expert(index):
        picks = lax.dynamic_slice_in_dim(table, index * per_expert, per_expert, 0)
        live = lax.dynamic_slice_in_dim(filled, index * per_expert, per_expert, 0)
        rows = normed[picks] * live[:, None].astype(normed.dtype)
        gate = jnp.dot(rows, gate_w[index], preferred_element_type=jnp.float32)
        upper = jnp.dot(rows, up_w[index], preferred_element_type=jnp.float32)
        hidden = (jax.nn.silu(gate) * upper).astype(jnp.bfloat16)
        return jnp.dot(hidden, down_w[index], preferred_element_type=jnp.float32).astype(jnp.bfloat16)
    results = lax.map(one_expert, jnp.arange(EXPERTS, dtype=jnp.int32))
    flat_out = results.reshape(EXPERTS * per_expert, D)
    chosen = flat_out[where_to].reshape(TOKENS, TOP, D).astype(jnp.float32)
    return lax.optimization_barrier(jnp.sum(chosen * route_weight[:, :, None], axis=1))

def reference(query_a, key_a, value_a, cumlog_a, query_b, key_b, value_b, cumlog_b, out_weight_a, out_weight_b, residual, norm_gain, expert_ids, route_weight, gate_w, up_w, down_w):
    attn_a = attend_group(query_a, key_a, value_a, cumlog_a, HA, HDA)
    attn_b = attend_group(query_b, key_b, value_b, cumlog_b, HB, HDB)
    mixed = project_out(attn_a, attn_b, out_weight_a, out_weight_b)
    summed = residual.astype(jnp.float32) + mixed
    center = summed - lax.optimization_barrier(jnp.mean(summed, axis=-1, keepdims=True))
    variance = lax.optimization_barrier(jnp.mean(center * center, axis=-1, keepdims=True))
    normed = (center * lax.rsqrt(variance + norm_eps) * norm_gain).astype(jnp.bfloat16)
    routed = experts_out(normed, expert_ids, route_weight, gate_w, up_w, down_w)
    return (normed.astype(jnp.float32) + routed).astype(jnp.bfloat16)
```

```python
import functools

import jax
import jax.numpy as jnp
from jax import lax
from jax.experimental import pallas as pl
from jax.experimental.pallas import tpu as pltpu
from jax.sharding import PartitionSpec as P

HDA = 64
HDB = 128
GROUPS = 4
TOP = 2


norm_eps = 1e-05


def fold_group(state, queries, keys_piece, values_piece, cum_query, cum_key, visible, head_size):
    best, total, accum = state
    heads = best.shape[0]
    count = keys_piece.shape[1]
    key_grid = keys_piece.reshape(heads, head_size, count)
    value_grid = values_piece.reshape(heads, head_size, count)
    scores = jnp.einsum(
        "hdq,hdk->hqk", queries, key_grid, preferred_element_type=jnp.float32
    ) * head_size ** (-0.5)
    scores = scores + cum_query[:, :, None] - cum_key[:, None, :]
    scores = jnp.where(visible, scores, -jnp.inf)
    best_new = jnp.max(scores, axis=-1)
    shift = jnp.where(best_new > -jnp.inf, best_new, 0.0)
    keep_old = jnp.exp(best - shift)
    weights = jnp.exp(scores - shift[:, :, None])
    total_new = total * keep_old + jnp.sum(weights, axis=-1)
    added = jnp.einsum(
        "hqk,hdk->hdq", weights.astype(jnp.bfloat16), value_grid, preferred_element_type=jnp.float32
    )
    return (best_new, total_new, accum * keep_old[:, None, :] + added)


def empty_state(heads, head_size, length):
    return (
        jnp.full((heads, length), -jnp.inf, jnp.float32),
        jnp.zeros((heads, length), jnp.float32),
        jnp.zeros((heads, head_size, length), jnp.float32),
    )


def finish_state(state):
    accum = state[2] / state[1][:, None, :]
    return accum.astype(jnp.bfloat16).reshape(-1, accum.shape[2])


def per_device(
    query_a,
    key_a,
    value_a,
    cumlog_a,
    query_b,
    key_b,
    value_b,
    cumlog_b,
    out_weight_a,
    out_weight_b,
    residual,
    norm_gain,
    expert_ids,
    route_weight,
    gate_w,
    up_w,
    down_w,
):
    local_tokens = query_a.shape[1]
    heads_a = cumlog_a.shape[0]
    heads_b = cumlog_b.shape[0]
    my_start = lax.axis_index("sp") * local_tokens
    last_query = my_start + local_tokens - 1
    query_pos = my_start + jnp.arange(local_tokens, dtype=jnp.int32)
    cum_query_a = lax.dynamic_slice_in_dim(cumlog_a, my_start, local_tokens, 1)
    cum_query_b = lax.dynamic_slice_in_dim(cumlog_b, my_start, local_tokens, 1)
    grid_a = query_a.reshape(heads_a, HDA, local_tokens)
    grid_b = query_b.reshape(heads_b, HDB, local_tokens)
    keys_a = lax.all_gather(key_a, "sp", axis=1, tiled=True)
    vals_a = lax.all_gather(value_a, "sp", axis=1, tiled=True)
    keys_b = lax.all_gather(key_b, "sp", axis=1, tiled=True)
    vals_b = lax.all_gather(value_b, "sp", axis=1, tiled=True)
    count = keys_a.shape[1]

    def visit(state):
        key_pos = jnp.arange(count, dtype=jnp.int32)
        visible = key_pos[None, None, :] <= query_pos[None, :, None]
        new_a = fold_group(state[0], grid_a, keys_a, vals_a, cum_query_a, cumlog_a, visible, HDA)
        new_b = fold_group(state[1], grid_b, keys_b, vals_b, cum_query_b, cumlog_b, visible, HDB)
        return (new_a, new_b)

    def leave(state):
        return state

    state_a, state_b = lax.cond(
        jnp.int32(0) <= last_query,
        visit,
        leave,
        (empty_state(heads_a, HDA, local_tokens), empty_state(heads_b, HDB, local_tokens)),
    )
    attn_a = finish_state(state_a)
    attn_b = finish_state(state_b)
    term = lax.dot_general(
        attn_a, out_weight_a, (((0,), (0,)), ((), ())), preferred_element_type=jnp.float32
    )
    mixed = lax.psum_scatter(
        (
            term
            + lax.dot_general(
                attn_b, out_weight_b, (((0,), (0,)), ((), ())), preferred_element_type=jnp.float32
            )
        ).astype(jnp.bfloat16),
        "tp",
        scatter_dimension=0,
        tiled=True,
    ).astype(jnp.float32)
    summed = residual.astype(jnp.float32) + mixed
    center = summed - jnp.mean(summed, axis=-1, keepdims=True)
    variance = jnp.mean(center * center, axis=-1, keepdims=True)
    normed = (center * lax.rsqrt(variance + norm_eps) * norm_gain).astype(jnp.bfloat16)
    normed_all = lax.all_gather(normed, "tp", axis=0, tiled=True)
    experts = lax.axis_size("sp")
    group_size = experts // GROUPS
    capacity = local_tokens // group_size
    features = normed_all.shape[1]
    flat_ids = expert_ids.reshape(-1)
    marks = (flat_ids[:, None] == jnp.arange(experts, dtype=jnp.int32)[None, :]).astype(jnp.int32)
    rank = jnp.sum((jnp.cumsum(marks, axis=0) - marks) * marks, axis=1)
    slot = flat_ids * capacity + rank
    token_of = jnp.arange(local_tokens * TOP, dtype=jnp.int32) // TOP
    table = jnp.zeros((experts * capacity,), jnp.int32).at[slot].set(token_of)
    filled = jnp.zeros((experts * capacity,), jnp.bfloat16).at[slot].set(1.0)
    send = (normed_all[table] * filled[:, None]).reshape(experts, capacity, features)
    rows = lax.all_to_all(send, "sp", split_axis=0, concat_axis=0, tiled=True)
    sources, items, row_width = rows.shape
    flat_rows = rows.reshape(sources * items, row_width)
    gate = jnp.dot(flat_rows, gate_w[0], preferred_element_type=jnp.float32)
    upper = jnp.dot(flat_rows, up_w[0], preferred_element_type=jnp.float32)
    hidden = (jax.nn.silu(gate) * upper).astype(jnp.bfloat16).reshape(sources, items, -1)
    hidden_all = lax.all_gather(hidden, "tp", axis=2, tiled=True)
    result = jnp.dot(
        hidden_all.reshape(sources * items, -1), down_w[0], preferred_element_type=jnp.float32
    )
    result = result.astype(jnp.bfloat16).reshape(sources, items, -1)
    returned = lax.all_to_all(result, "sp", split_axis=0, concat_axis=0, tiled=True)
    flat_back = returned.reshape(experts * capacity, -1)
    picked = flat_back[slot].reshape(local_tokens, TOP, -1).astype(jnp.float32)
    routed = jnp.sum(picked * route_weight[:, :, None], axis=1)
    columns = routed.shape[1]
    own_cols = lax.dynamic_slice_in_dim(normed_all, lax.axis_index("tp") * columns, columns, 1)
    return (own_cols.astype(jnp.float32) + routed).astype(jnp.bfloat16)


MESH = pl.DeviceIdType.MESH
F32 = jnp.float32
BF16 = jnp.bfloat16


def fused_kernel(
    dims,
    q_a, k_a, v_a, cum_a, q_b, k_b, v_b, cum_b, residual, gain, ids, route,
    wa_hbm, wb_hbm, gate_hbm, up_hbm, down_hbm,
    out,
    wa, wb, gw, uw, dw,
    got_a, got_b, cols, mine_a, mine_b, att_a, att_b,
    ps, rs, nb, nf, onehot, wsend, wgot, dsend, xs, hid, own, part_send, part_got, ret_send, ret,
    w_sem, qkv_send, qkv_recv, att_send, att_recv, rs_send, rs_recv, nf_send, nf_recv,
    ws_send, ws_recv, d_send, d_recv, ag_send, ag_recv, pair_send, pair_recv,
    h_send, h_recv, e_send, e_recv, r_send, r_recv,
):
    n_sp, n_tp, heads_a, da, db, group_size = dims
    s = lax.axis_index("sp")
    t = lax.axis_index("tp")
    z = s // 2
    c = s % 2
    nz = n_sp // 2
    tok = q_a.shape[1]
    groups = nz
    slots = dsend.shape[1]
    sub = tok // n_tp
    feat = nf.shape[1]

    def tp_to(j):
        if n_tp == 4:
            return {1: t + 1 - 2 * (t % 2), 2: (t + 2) % 4, 3: 3 - t}[j]
        return (t + j) % n_tp

    def tp_from(j):
        if n_tp == 4:
            return tp_to(j)
        return (t + n_tp - j) % n_tp

    def remote(src, dst, send, recv, sp, tp):
        return pltpu.make_async_remote_copy(
            src_ref=src, dst_ref=dst, send_sem=send, recv_sem=recv,
            device_id={"sp": sp, "tp": tp}, device_id_type=MESH,
        )

    loads = []
    for i, (src, dst) in enumerate(
        ((wa_hbm, wa), (wb_hbm, wb), (gate_hbm.at[0], gw), (up_hbm.at[0], uw), (down_hbm.at[0], dw))
    ):
        copy = pltpu.make_async_copy(src, dst, w_sem.at[i])
        copy.start()
        loads.append(copy)

    barrier = pltpu.get_barrier_semaphore()
    for k in range(1, n_sp):
        pl.semaphore_signal(
            barrier, inc=1, device_id={"sp": (s + k) % n_sp, "tp": t}, device_id_type=MESH
        )
    for j in range(1, n_tp):
        pl.semaphore_signal(
            barrier, inc=1, device_id={"sp": s, "tp": tp_to(j)}, device_id_type=MESH
        )
    pl.semaphore_wait(barrier, n_sp - 1 + n_tp - 1)

    sources = ((q_a, k_a, v_a), (q_b, k_b, v_b))
    got = (got_a, got_b)
    sizes = (da, db)

    def qkv_copies(core):
        copies = []
        for k in range(1, n_sp):
            target = (s + k) % n_sp
            kind = (core + k) % 2
            d = sizes[kind]
            rows = pl.ds(pl.multiple_of((target // 2) * d, d), d)
            for m in range(3):
                copies.append(remote(
                    sources[kind][m].at[rows], got[kind].at[m, s],
                    qkv_send.at[m, k], qkv_recv.at[m, s], target, t,
                ))
        return copies

    for core in range(2):
        @pl.when(c == core)
        def _(core=core):
            for copy in qkv_copies(core):
                copy.start()
            d = sizes[core]
            rows = pl.ds(pl.multiple_of(z * d, d), d)
            for m in range(3):
                got[core][m, s] = sources[core][m][rows, :]

    ids_v = ids[...].astype(F32)
    id0 = ids_v[:, 0:1]
    lane = lax.broadcasted_iota(jnp.int32, (tok, 128), 1).astype(F32)
    first = lane * group_size
    member = (id0 >= first) & (id0 < first + group_size) & (lane < groups)
    member = jnp.where(member, 1.0, 0.0)
    low = lax.broadcasted_iota(jnp.int32, (tok, tok), 1) < lax.broadcasted_iota(jnp.int32, (tok, tok), 0)
    rank = jnp.dot(
        jnp.where(low, 1.0, 0.0).astype(BF16), member.astype(BF16), preferred_element_type=F32
    )
    slot = jnp.sum(member * (rank + lane * slots), axis=1, keepdims=True)
    base = jnp.sum(member * first, axis=1, keepdims=True)
    wide = lax.broadcasted_iota(jnp.int32, (tok, groups * slots), 1).astype(F32)
    pick = jnp.where(wide == slot, 1.0, 0.0)
    onehot[...] = pick.astype(BF16)
    spread = jnp.transpose(pick).astype(BF16)
    even = id0 == base
    r0 = route[:, 0:1]
    r1 = route[:, 1:2]
    w_even = jnp.where(even, r0, r1)
    w_odd = jnp.where(even, r1, r0)
    w_lanes = jnp.where(lane == 0.0, w_even, jnp.where(lane == 1.0, w_odd, 0.0))
    hi = w_lanes.astype(BF16)
    rest = w_lanes - hi.astype(F32)
    mid = rest.astype(BF16)
    tail = (rest - mid.astype(F32)).astype(BF16)
    w_slots = (
        jnp.dot(spread, hi, preferred_element_type=F32)
        + jnp.dot(spread, mid, preferred_element_type=F32)
        + jnp.dot(spread, tail, preferred_element_type=F32)
    )
    wsend[...] = w_slots.reshape(groups, slots, 128)
    wgot[z] = wsend[z]
    w_copies = []
    for k in range(1, nz):
        zt = (z + k) % nz
        copy = remote(wsend.at[zt], wgot.at[z], ws_send.at[k], ws_recv.at[k], 2 * zt + c, t)
        copy.start()
        w_copies.append(copy)

    span = 2 * tok
    mine = (mine_a, mine_b)
    att = (att_a, att_b)
    cums = (cum_a, cum_b)

    def att_copy(core, dest):
        d = sizes[core]
        rows = pl.ds(pl.multiple_of(z * d, d), d)
        return remote(
            mine[core].at[dest], att[core].at[rows], att_send.at[dest], att_recv.at[s], dest, t
        )

    def attend(core):
        d = sizes[core]
        ref = got[core]
        row = cums[core][pl.ds(z, 1), :]
        for j in range(n_sp):
            part = row[:, j * tok:(j + 1) * tok]
            cols[pl.ds(j * tok, tok), :] = jnp.transpose(jnp.broadcast_to(part, (tok, tok)))
        scale = d ** (-0.5)
        keys_t = []
        values = []
        for step in range(n_sp // 2):
            for src in (2 * step, 2 * step + 1):
                @pl.when(s != src)
                def _(src=src):
                    for m in range(3):
                        remote(
                            ref.at[m, src], ref.at[m, src],
                            qkv_send.at[m, 0], qkv_recv.at[m, src], src, t,
                        ).wait_recv()
            for src in (2 * step, 2 * step + 1):
                keys_t.append(jnp.transpose(ref[1, src]))
                values.append(ref[2, src])
            queries = jnp.concatenate([ref[0, 2 * step], ref[0, 2 * step + 1]], axis=1)
            count = span * (step + 1)
            keys = jnp.concatenate(keys_t, axis=0)
            vals = jnp.concatenate(values, axis=1)
            score = jnp.dot(keys, queries, preferred_element_type=F32) * scale
            cum_k = cols[pl.ds(0, count), :]
            cum_q = row[:, step * span:(step + 1) * span]
            score = score + (cum_q - jnp.concatenate([cum_k, cum_k], axis=1))
            k_at = lax.broadcasted_iota(jnp.int32, (count, span), 0)
            q_at = lax.broadcasted_iota(jnp.int32, (count, span), 1) + step * span
            score = jnp.where(k_at <= q_at, score, -jnp.inf)
            best = jnp.max(score, axis=0, keepdims=True)
            weight = jnp.exp(score - best)
            total = jnp.sum(weight, axis=0, keepdims=True)
            res = jnp.dot(vals, weight.astype(BF16), preferred_element_type=F32) / total
            res = res.astype(BF16)
            for half in range(2):
                dest = 2 * step + half
                mine[core][dest] = res[:, half * tok:(half + 1) * tok]

                @pl.when(s != dest)
                def _(dest=dest):
                    att_copy(core, dest).start()

                @pl.when(s == dest)
                def _(dest=dest):
                    att[core][pl.ds(pl.multiple_of(z * d, d), d), :] = mine[core][dest]

    for core in range(2):
        @pl.when(c == core)
        def _(core=core):
            attend(core)

    for src in range(n_sp):
        core = src % 2
        d = sizes[core]

        @pl.when(s != src)
        def _(src=src, core=core, d=d):
            part = att[core].at[pl.ds((src // 2) * d, d)]
            remote(part, part, att_send.at[src], att_recv.at[src], src, t).wait_recv()

    loads[0].wait()
    loads[1].wait()
    left_a = jnp.transpose(att_a[...])
    left_b = jnp.transpose(att_b[...])
    pieces = ps.shape[0]
    width = ps.shape[2]
    rs_copies = []
    for ch in range(pieces):
        at = pl.ds(ch * width, width)
        term = jnp.dot(left_a, wa[:, at], preferred_element_type=F32)
        term = term + jnp.dot(left_b, wb[:, at], preferred_element_type=F32)
        ps[ch] = term.astype(BF16)
        for j in range(1, n_tp):
            to = tp_to(j)
            copy = remote(
                ps.at[ch, pl.ds(pl.multiple_of(to * sub, sub), sub)], rs.at[ch, j - 1],
                rs_send.at[ch, j - 1], rs_recv.at[ch, j - 1], s, to,
            )
            copy.start()
            rs_copies.append(copy)
    sums = []
    for ch in range(pieces):
        at = pl.ds(ch * width, width)
        value = residual[:, at].astype(F32) + ps[
            ch, pl.ds(pl.multiple_of(t * sub, sub), sub), :
        ].astype(F32)
        for j in range(1, n_tp):
            rs_copies[ch * (n_tp - 1) + j - 1].wait_recv()
            value = value + rs[ch, j - 1].astype(F32)
        sums.append(value)
    summed = jnp.concatenate(sums, axis=1)
    center = summed - jnp.mean(summed, axis=-1, keepdims=True)
    variance = jnp.mean(center * center, axis=-1, keepdims=True)
    normed = (center * lax.rsqrt(variance + norm_eps) * gain[...]).astype(BF16)
    for i in range(n_tp):
        nb[i] = normed[:, i * feat:(i + 1) * feat]
    here = pl.ds(pl.multiple_of(t * sub, sub), sub)
    nf_copies = []
    for j in range(1, n_tp):
        to = tp_to(j)
        copy = remote(nb.at[to], nf.at[here], nf_send.at[j - 1], nf_recv.at[j - 1], s, to)
        copy.start()
        nf_copies.append(copy)
    nf[here, :] = nb[t]
    for copy in nf_copies:
        copy.wait_recv()

    spread = jnp.transpose(onehot[...].astype(F32)).astype(BF16)
    dsend[...] = jnp.dot(spread, nf[...], preferred_element_type=F32).astype(BF16).reshape(
        groups, slots, feat
    )
    d_copies = []
    for k in range(1, nz):
        zt = (z + k) % nz
        copy = remote(dsend.at[zt], xs.at[c, t, z], d_send.at[k], d_recv.at[k], 2 * zt + c, t)
        copy.start()
        d_copies.append(copy)
    xs[c, t, z] = dsend[z]
    mate = 2 * z + 1 - c
    ag_copies = []
    pair_copies = []
    for k in range(nz):
        zs = (z + nz - k) % nz
        if k:
            d_copies[k - 1].wait_recv()
        block = xs.at[c, t, zs]
        row = []
        for j in range(1, n_tp):
            copy = remote(block, block, ag_send.at[j - 1, k], ag_recv.at[j - 1, k], s, tp_to(j))
            copy.start()
            row.append(copy)
        ag_copies.append(row)
        copy = remote(block, block, pair_send.at[0, k], pair_recv.at[0, k], mate, t)
        copy.start()
        pair_copies.append([copy])

    loads[2].wait()
    loads[3].wait()
    h_copies = []
    for k in range(nz):
        zs = (z + nz - k) % nz
        for j in range(1, n_tp):
            ag_copies[k][j - 1].wait_recv()
            block = xs.at[c, tp_from(j), zs]
            copy = remote(block, block, pair_send.at[j, k], pair_recv.at[j, k], mate, t)
            copy.start()
            pair_copies[k].append(copy)
        for j in range(n_tp):
            pair_copies[k][j].wait_recv()
        rows = [
            jnp.concatenate([xs[0, i, zs], xs[1, i, zs]], axis=0) for i in range(n_tp)
        ]
        rows = jnp.concatenate(rows, axis=1)
        gate = jnp.dot(rows, gw[...], preferred_element_type=F32)
        upper = jnp.dot(rows, uw[...], preferred_element_type=F32)
        hid[zs, t] = (gate / (1.0 + jnp.exp(-gate)) * upper).astype(BF16)
        block = hid.at[zs, t]
        row = []
        for j in range(1, n_tp):
            copy = remote(block, block, h_send.at[j - 1, k], h_recv.at[j - 1, k], s, tp_to(j))
            copy.start()
            row.append(copy)
        h_copies.append(row)

    loads[4].wait()
    e_copies = []
    for k in range(nz):
        zs = (z + nz - k) % nz
        for copy in h_copies[k]:
            copy.wait_recv()
        rows = jnp.concatenate([hid[zs, i] for i in range(n_tp)], axis=1)
        result = jnp.dot(rows, dw[...], preferred_element_type=F32)
        top = result[:slots]
        bottom = result[slots:]
        own[zs] = jnp.where(c == 0, top, bottom)
        part_send[zs] = jnp.where(c == 0, bottom, top).astype(BF16)
        copy = remote(part_send.at[zs], part_got.at[zs], e_send.at[k], e_recv.at[k], mate, t)
        copy.start()
        e_copies.append(copy)

    r_copies = []
    for k in range(nz):
        zs = (z + nz - k) % nz
        if k:
            w_copies[k - 1].wait_recv()
        e_copies[k].wait_recv()
        both = wgot[zs]
        w0 = both[:, 0:1]
        w1 = both[:, 1:2]
        own_w = jnp.where(c == 0, w0, w1)
        mate_w = jnp.where(c == 0, w1, w0)
        total = (own_w * own[zs] + mate_w * part_got[zs].astype(F32)).astype(BF16)
        if k:
            ret_send[k] = total
            copy = remote(
                ret_send.at[k], ret.at[pl.ds(pl.multiple_of(z * slots, slots), slots)],
                r_send.at[k], r_recv.at[k], 2 * zs + c, t,
            )
            copy.start()
            r_copies.append(copy)
        else:
            ret[pl.ds(pl.multiple_of(z * slots, slots), slots), :] = total

    for k in range(1, nz):
        r_copies[k - 1].wait_recv()
    routed = jnp.dot(onehot[...], ret[...], preferred_element_type=F32)
    out[...] = (nf[...].astype(F32) + routed).astype(BF16)

    for core in range(2):
        @pl.when(c == core)
        def _(core=core):
            for copy in qkv_copies(core):
                copy.wait_send()
            for dest in range(n_sp):
                @pl.when(s != dest)
                def _(dest=dest):
                    att_copy(core, dest).wait_send()
    flat = w_copies + rs_copies + nf_copies + d_copies + e_copies + r_copies
    for group in (ag_copies, pair_copies, h_copies):
        for row in group:
            flat = flat + row
    for copy in flat:
        copy.wait_send()


def fused(
    query_a, key_a, value_a, cumlog_a, query_b, key_b, value_b, cumlog_b, out_weight_a,
    out_weight_b, residual, norm_gain, expert_ids, route_weight, gate_w, up_w, down_w,
):
    n_sp = lax.axis_size("sp")
    n_tp = lax.axis_size("tp")
    nz = n_sp // 2
    tok = query_a.shape[1]
    sub = tok // n_tp
    model = residual.shape[1]
    feat = down_w.shape[2]
    inner = gate_w.shape[2]
    group_size = n_sp // GROUPS
    slots = tok // TOP
    pieces = 2
    width = model // pieces
    dims = (n_sp, n_tp, cumlog_a.shape[0], HDA, HDB, group_size)
    vmem = pl.BlockSpec(memory_space=pltpu.VMEM)
    anyw = pl.BlockSpec(memory_space=pl.ANY)
    dma = pltpu.SemaphoreType.DMA
    scratch = [
        pltpu.VMEM(out_weight_a.shape, BF16),
        pltpu.VMEM(out_weight_b.shape, BF16),
        pltpu.VMEM(gate_w.shape[1:], BF16),
        pltpu.VMEM(up_w.shape[1:], BF16),
        pltpu.VMEM(down_w.shape[1:], BF16),
        pltpu.VMEM((3, n_sp, HDA, tok), BF16),
        pltpu.VMEM((3, n_sp, HDB, tok), BF16),
        pltpu.VMEM((n_sp * tok, tok), F32),
        pltpu.VMEM((n_sp, HDA, tok), BF16),
        pltpu.VMEM((n_sp, HDB, tok), BF16),
        pltpu.VMEM(query_a.shape, BF16),
        pltpu.VMEM(query_b.shape, BF16),
        pltpu.VMEM((pieces, tok, width), BF16),
        pltpu.VMEM((pieces, n_tp - 1, sub, width), BF16),
        pltpu.VMEM((n_tp, sub, feat), BF16),
        pltpu.VMEM((tok, feat), BF16),
        pltpu.VMEM((tok, nz * slots), BF16),
        pltpu.VMEM((nz, slots, 128), F32),
        pltpu.VMEM((nz, slots, 128), F32),
        pltpu.VMEM((nz, slots, feat), BF16),
        pltpu.VMEM((2, n_tp, nz, slots, feat), BF16),
        pltpu.VMEM((nz, n_tp, 2 * slots, inner), BF16),
        pltpu.VMEM((nz, slots, feat), F32),
        pltpu.VMEM((nz, slots, feat), BF16),
        pltpu.VMEM((nz, slots, feat), BF16),
        pltpu.VMEM((nz, slots, feat), BF16),
        pltpu.VMEM((nz * slots, feat), BF16),
        dma((5,)),
        dma((3, n_sp)), dma((3, n_sp)),
        dma((n_sp,)), dma((n_sp,)),
        dma((pieces, n_tp - 1)), dma((pieces, n_tp - 1)),
        dma((n_tp - 1,)), dma((n_tp - 1,)),
        dma((nz,)), dma((nz,)),
        dma((nz,)), dma((nz,)),
        dma((n_tp - 1, nz)), dma((n_tp - 1, nz)),
        dma((n_tp, nz)), dma((n_tp, nz)),
        dma((n_tp - 1, nz)), dma((n_tp - 1, nz)),
        dma((nz,)), dma((nz,)),
        dma((nz,)), dma((nz,)),
    ]
    return pl.pallas_call(
        functools.partial(fused_kernel, dims),
        out_shape=jax.ShapeDtypeStruct((tok, feat), BF16),
        in_specs=[vmem] * 12 + [anyw] * 5,
        out_specs=vmem,
        scratch_shapes=scratch,
        compiler_params=pltpu.CompilerParams(
            collective_id=0, has_side_effects=True, vmem_limit_bytes=48 * 1024 * 1024
        ),
    )(
        query_a, key_a, value_a, cumlog_a, query_b, key_b, value_b, cumlog_b, residual,
        norm_gain.reshape(1, -1), expert_ids, route_weight, out_weight_a, out_weight_b,
        gate_w, up_w, down_w,
    )


def choose(*args):
    n_sp = lax.axis_size("sp")
    heads_a = args[3].shape[0]
    heads_b = args[7].shape[0]
    fits = heads_a == heads_b and heads_a + heads_b == n_sp
    fits = fits and n_sp == GROUPS * TOP and n_sp == 2 * GROUPS
    return (fused if fits else per_device)(*args)


def solution(mesh):
    placed = (
        P("tp", "sp"),
        P("tp", "sp"),
        P("tp", "sp"),
        P("tp", None),
        P("tp", "sp"),
        P("tp", "sp"),
        P("tp", "sp"),
        P("tp", None),
        P("tp", None),
        P("tp", None),
        P(("sp", "tp"), None),
        P(),
        P("sp", None),
        P("sp", None),
        P("sp", None, "tp"),
        P("sp", None, "tp"),
        P("sp", None, "tp"),
    )
    return jax.shard_map(
        choose, mesh=mesh, in_specs=placed, out_specs=P("sp", "tp"), check_vma=False
    )
```

```python
import functools

import jax
import jax.numpy as jnp
from jax import lax
from jax.experimental import pallas as pl
from jax.experimental.pallas import tpu as pltpu
from jax.sharding import PartitionSpec as P

HDA = 64
HDB = 128
GROUPS = 4
TOP = 2


norm_eps = 1e-05


def fold_group(state, queries, keys_piece, values_piece, cum_query, cum_key, visible, head_size):
    best, total, accum = state
    heads = best.shape[0]
    count = keys_piece.shape[1]
    key_grid = keys_piece.reshape(heads, head_size, count)
    value_grid = values_piece.reshape(heads, head_size, count)
    scores = jnp.einsum(
        "hdq,hdk->hqk", queries, key_grid, preferred_element_type=jnp.float32
    ) * head_size ** (-0.5)
    scores = scores + cum_query[:, :, None] - cum_key[:, None, :]
    scores = jnp.where(visible, scores, -jnp.inf)
    best_new = jnp.max(scores, axis=-1)
    shift = jnp.where(best_new > -jnp.inf, best_new, 0.0)
    keep_old = jnp.exp(best - shift)
    weights = jnp.exp(scores - shift[:, :, None])
    total_new = total * keep_old + jnp.sum(weights, axis=-1)
    added = jnp.einsum(
        "hqk,hdk->hdq", weights.astype(jnp.bfloat16), value_grid, preferred_element_type=jnp.float32
    )
    return (best_new, total_new, accum * keep_old[:, None, :] + added)


def empty_state(heads, head_size, length):
    return (
        jnp.full((heads, length), -jnp.inf, jnp.float32),
        jnp.zeros((heads, length), jnp.float32),
        jnp.zeros((heads, head_size, length), jnp.float32),
    )


def finish_state(state):
    accum = state[2] / state[1][:, None, :]
    return accum.astype(jnp.bfloat16).reshape(-1, accum.shape[2])


def per_device(
    query_a,
    key_a,
    value_a,
    cumlog_a,
    query_b,
    key_b,
    value_b,
    cumlog_b,
    out_weight_a,
    out_weight_b,
    residual,
    norm_gain,
    expert_ids,
    route_weight,
    gate_w,
    up_w,
    down_w,
):
    local_tokens = query_a.shape[1]
    heads_a = cumlog_a.shape[0]
    heads_b = cumlog_b.shape[0]
    my_start = lax.axis_index("sp") * local_tokens
    last_query = my_start + local_tokens - 1
    query_pos = my_start + jnp.arange(local_tokens, dtype=jnp.int32)
    cum_query_a = lax.dynamic_slice_in_dim(cumlog_a, my_start, local_tokens, 1)
    cum_query_b = lax.dynamic_slice_in_dim(cumlog_b, my_start, local_tokens, 1)
    grid_a = query_a.reshape(heads_a, HDA, local_tokens)
    grid_b = query_b.reshape(heads_b, HDB, local_tokens)
    keys_a = lax.all_gather(key_a, "sp", axis=1, tiled=True)
    vals_a = lax.all_gather(value_a, "sp", axis=1, tiled=True)
    keys_b = lax.all_gather(key_b, "sp", axis=1, tiled=True)
    vals_b = lax.all_gather(value_b, "sp", axis=1, tiled=True)
    count = keys_a.shape[1]

    def visit(state):
        key_pos = jnp.arange(count, dtype=jnp.int32)
        visible = key_pos[None, None, :] <= query_pos[None, :, None]
        new_a = fold_group(state[0], grid_a, keys_a, vals_a, cum_query_a, cumlog_a, visible, HDA)
        new_b = fold_group(state[1], grid_b, keys_b, vals_b, cum_query_b, cumlog_b, visible, HDB)
        return (new_a, new_b)

    def leave(state):
        return state

    state_a, state_b = lax.cond(
        jnp.int32(0) <= last_query,
        visit,
        leave,
        (empty_state(heads_a, HDA, local_tokens), empty_state(heads_b, HDB, local_tokens)),
    )
    attn_a = finish_state(state_a)
    attn_b = finish_state(state_b)
    term = lax.dot_general(
        attn_a, out_weight_a, (((0,), (0,)), ((), ())), preferred_element_type=jnp.float32
    )
    mixed = lax.psum_scatter(
        (
            term
            + lax.dot_general(
                attn_b, out_weight_b, (((0,), (0,)), ((), ())), preferred_element_type=jnp.float32
            )
        ).astype(jnp.bfloat16),
        "tp",
        scatter_dimension=0,
        tiled=True,
    ).astype(jnp.float32)
    summed = residual.astype(jnp.float32) + mixed
    center = summed - jnp.mean(summed, axis=-1, keepdims=True)
    variance = jnp.mean(center * center, axis=-1, keepdims=True)
    normed = (center * lax.rsqrt(variance + norm_eps) * norm_gain).astype(jnp.bfloat16)
    normed_all = lax.all_gather(normed, "tp", axis=0, tiled=True)
    experts = lax.axis_size("sp")
    group_size = experts // GROUPS
    capacity = local_tokens // group_size
    features = normed_all.shape[1]
    flat_ids = expert_ids.reshape(-1)
    marks = (flat_ids[:, None] == jnp.arange(experts, dtype=jnp.int32)[None, :]).astype(jnp.int32)
    rank = jnp.sum((jnp.cumsum(marks, axis=0) - marks) * marks, axis=1)
    slot = flat_ids * capacity + rank
    token_of = jnp.arange(local_tokens * TOP, dtype=jnp.int32) // TOP
    table = jnp.zeros((experts * capacity,), jnp.int32).at[slot].set(token_of)
    filled = jnp.zeros((experts * capacity,), jnp.bfloat16).at[slot].set(1.0)
    send = (normed_all[table] * filled[:, None]).reshape(experts, capacity, features)
    rows = lax.all_to_all(send, "sp", split_axis=0, concat_axis=0, tiled=True)
    sources, items, row_width = rows.shape
    flat_rows = rows.reshape(sources * items, row_width)
    gate = jnp.dot(flat_rows, gate_w[0], preferred_element_type=jnp.float32)
    upper = jnp.dot(flat_rows, up_w[0], preferred_element_type=jnp.float32)
    hidden = (jax.nn.silu(gate) * upper).astype(jnp.bfloat16).reshape(sources, items, -1)
    hidden_all = lax.all_gather(hidden, "tp", axis=2, tiled=True)
    result = jnp.dot(
        hidden_all.reshape(sources * items, -1), down_w[0], preferred_element_type=jnp.float32
    )
    result = result.astype(jnp.bfloat16).reshape(sources, items, -1)
    returned = lax.all_to_all(result, "sp", split_axis=0, concat_axis=0, tiled=True)
    flat_back = returned.reshape(experts * capacity, -1)
    picked = flat_back[slot].reshape(local_tokens, TOP, -1).astype(jnp.float32)
    routed = jnp.sum(picked * route_weight[:, :, None], axis=1)
    columns = routed.shape[1]
    own_cols = lax.dynamic_slice_in_dim(normed_all, lax.axis_index("tp") * columns, columns, 1)
    return (own_cols.astype(jnp.float32) + routed).astype(jnp.bfloat16)


MESH = pl.DeviceIdType.MESH
F32 = jnp.float32
BF16 = jnp.bfloat16


def fused_kernel(
    dims,
    q_a_hbm, k_a_hbm, v_a_hbm, cum_a_hbm, q_b_hbm, k_b_hbm, v_b_hbm, cum_b_hbm,
    residual_hbm, gain_hbm, ids_hbm, route_hbm,
    wa_hbm, wb_hbm, gate_hbm, up_hbm, down_hbm,
    out,
    q_a, k_a, v_a, cum_a, q_b, k_b, v_b, cum_b, residual, gain, ids, route,
    wa, wb, gw, uw, dw,
    got_a, got_b, cols, mine_a, mine_b, att_a, att_b,
    ps, rs, nb, nf, onehot, wsend, wgot, dsend, xs, hid, own, part_send, part_got, ret_send, ret,
    w_sem, qkv_send, qkv_recv, att_send, att_recv, rs_send, rs_recv, nf_send, nf_recv,
    ws_send, ws_recv, d_send, d_recv, ag_send, ag_recv, pair_send, pair_recv,
    h_send, h_recv, e_send, e_recv, r_send, r_recv,
):
    n_sp, n_tp, heads_a, da, db, group_size = dims
    s = lax.axis_index("sp")
    t = lax.axis_index("tp")
    z = s // 2
    c = s % 2
    nz = n_sp // 2
    tok = q_a.shape[1]
    groups = nz
    slots = dsend.shape[1]
    sub = tok // n_tp
    feat = nf.shape[1]

    def tp_to(j):
        if n_tp == 4:
            return {1: t + 1 - 2 * (t % 2), 2: (t + 2) % 4, 3: 3 - t}[j]
        return (t + j) % n_tp

    def tp_from(j):
        if n_tp == 4:
            return tp_to(j)
        return (t + n_tp - j) % n_tp

    def remote(src, dst, send, recv, sp, tp):
        return pltpu.make_async_remote_copy(
            src_ref=src, dst_ref=dst, send_sem=send, recv_sem=recv,
            device_id={"sp": sp, "tp": tp}, device_id_type=MESH,
        )

    loads = []
    for i, (src, dst) in enumerate(
        (
            (q_a_hbm, q_a), (k_a_hbm, k_a), (v_a_hbm, v_a),
            (q_b_hbm, q_b), (k_b_hbm, k_b), (v_b_hbm, v_b),
            (ids_hbm, ids), (route_hbm, route), (cum_a_hbm, cum_a), (cum_b_hbm, cum_b),
            (wa_hbm, wa), (wb_hbm, wb), (residual_hbm, residual), (gain_hbm, gain),
            (gate_hbm.at[0], gw), (up_hbm.at[0], uw), (down_hbm.at[0], dw),
        )
    ):
        copy = pltpu.make_async_copy(src, dst, w_sem.at[i])
        copy.start()
        loads.append(copy)

    barrier = pltpu.get_barrier_semaphore()
    for k in range(1, n_sp):
        pl.semaphore_signal(
            barrier, inc=1, device_id={"sp": (s + k) % n_sp, "tp": t}, device_id_type=MESH
        )
    for j in range(1, n_tp):
        pl.semaphore_signal(
            barrier, inc=1, device_id={"sp": s, "tp": tp_to(j)}, device_id_type=MESH
        )
    pl.semaphore_wait(barrier, n_sp - 1 + n_tp - 1)

    for copy in loads[:6]:
        copy.wait()
    sources = ((q_a, k_a, v_a), (q_b, k_b, v_b))
    got = (got_a, got_b)
    sizes = (da, db)

    def qkv_copies(core):
        copies = []
        for k in range(1, n_sp):
            target = (s + k) % n_sp
            kind = (core + k) % 2
            d = sizes[kind]
            rows = pl.ds(pl.multiple_of((target // 2) * d, d), d)
            for m in range(3):
                copies.append(remote(
                    sources[kind][m].at[rows], got[kind].at[m, s],
                    qkv_send.at[m, k], qkv_recv.at[m, s], target, t,
                ))
        return copies

    for core in range(2):
        @pl.when(c == core)
        def _(core=core):
            for copy in qkv_copies(core):
                copy.start()
            d = sizes[core]
            rows = pl.ds(pl.multiple_of(z * d, d), d)
            for m in range(3):
                got[core][m, s] = sources[core][m][rows, :]

    loads[6].wait()
    loads[7].wait()

    def upright(row):
        return jnp.transpose(jnp.broadcast_to(row, (128, tok)))

    id0 = upright(ids[0:1, :].astype(F32))
    lane = lax.broadcasted_iota(jnp.int32, (tok, 128), 1).astype(F32)
    first = lane * group_size
    member = (id0 >= first) & (id0 < first + group_size) & (lane < groups)
    member = jnp.where(member, 1.0, 0.0)
    low = lax.broadcasted_iota(jnp.int32, (tok, tok), 1) < lax.broadcasted_iota(jnp.int32, (tok, tok), 0)
    rank = jnp.dot(
        jnp.where(low, 1.0, 0.0).astype(BF16), member.astype(BF16), preferred_element_type=F32
    )
    slot = jnp.sum(member * (rank + lane * slots), axis=1, keepdims=True)
    base = jnp.sum(member * first, axis=1, keepdims=True)
    wide = lax.broadcasted_iota(jnp.int32, (tok, groups * slots), 1).astype(F32)
    pick = jnp.where(wide == slot, 1.0, 0.0)
    onehot[...] = pick.astype(BF16)
    spread = jnp.transpose(pick).astype(BF16)
    even = id0 == base
    r0 = upright(route[0:1, :])
    r1 = upright(route[1:2, :])
    w_even = jnp.where(even, r0, r1)
    w_odd = jnp.where(even, r1, r0)
    w_lanes = jnp.where(lane == 0.0, w_even, jnp.where(lane == 1.0, w_odd, 0.0))
    hi = w_lanes.astype(BF16)
    rest = w_lanes - hi.astype(F32)
    mid = rest.astype(BF16)
    tail = (rest - mid.astype(F32)).astype(BF16)
    w_slots = (
        jnp.dot(spread, hi, preferred_element_type=F32)
        + jnp.dot(spread, mid, preferred_element_type=F32)
        + jnp.dot(spread, tail, preferred_element_type=F32)
    )
    wsend[...] = w_slots.reshape(groups, slots, 128)
    wgot[z] = wsend[z]
    w_copies = []
    for k in range(1, nz):
        zt = (z + k) % nz
        copy = remote(wsend.at[zt], wgot.at[z], ws_send.at[k], ws_recv.at[k], 2 * zt + c, t)
        copy.start()
        w_copies.append(copy)

    span = 2 * tok
    mine = (mine_a, mine_b)
    att = (att_a, att_b)
    cums = (cum_a, cum_b)

    def att_copy(core, dest):
        d = sizes[core]
        rows = pl.ds(pl.multiple_of(z * d, d), d)
        return remote(
            mine[core].at[dest], att[core].at[rows], att_send.at[dest], att_recv.at[s], dest, t
        )

    def attend(core):
        d = sizes[core]
        ref = got[core]
        loads[8 + core].wait()
        row = cums[core][pl.ds(z, 1), :]
        for j in range(n_sp):
            part = row[:, j * tok:(j + 1) * tok]
            cols[pl.ds(j * tok, tok), :] = jnp.transpose(jnp.broadcast_to(part, (tok, tok)))
        scale = d ** (-0.5)
        keys_t = []
        values = []
        for step in range(n_sp // 2):
            for src in (2 * step, 2 * step + 1):
                @pl.when(s != src)
                def _(src=src):
                    for m in range(3):
                        remote(
                            ref.at[m, src], ref.at[m, src],
                            qkv_send.at[m, 0], qkv_recv.at[m, src], src, t,
                        ).wait_recv()
            for src in (2 * step, 2 * step + 1):
                keys_t.append(jnp.transpose(ref[1, src]))
                values.append(ref[2, src])
            queries = jnp.concatenate([ref[0, 2 * step], ref[0, 2 * step + 1]], axis=1)
            count = span * (step + 1)
            keys = jnp.concatenate(keys_t, axis=0)
            vals = jnp.concatenate(values, axis=1)
            score = jnp.dot(keys, queries, preferred_element_type=F32) * scale
            cum_k = cols[pl.ds(0, count), :]
            cum_q = row[:, step * span:(step + 1) * span]
            score = score + (cum_q - jnp.concatenate([cum_k, cum_k], axis=1))
            k_at = lax.broadcasted_iota(jnp.int32, (count, span), 0)
            q_at = lax.broadcasted_iota(jnp.int32, (count, span), 1) + step * span
            score = jnp.where(k_at <= q_at, score, -jnp.inf)
            best = jnp.max(score, axis=0, keepdims=True)
            weight = jnp.exp(score - best)
            total = jnp.sum(weight, axis=0, keepdims=True)
            res = jnp.dot(vals, weight.astype(BF16), preferred_element_type=F32) / total
            res = res.astype(BF16)
            for half in range(2):
                dest = 2 * step + half
                mine[core][dest] = res[:, half * tok:(half + 1) * tok]

                @pl.when(s != dest)
                def _(dest=dest):
                    att_copy(core, dest).start()

                @pl.when(s == dest)
                def _(dest=dest):
                    att[core][pl.ds(pl.multiple_of(z * d, d), d), :] = mine[core][dest]

    for core in range(2):
        @pl.when(c == core)
        def _(core=core):
            attend(core)

    for src in range(n_sp):
        core = src % 2
        d = sizes[core]

        @pl.when(s != src)
        def _(src=src, core=core, d=d):
            part = att[core].at[pl.ds((src // 2) * d, d)]
            remote(part, part, att_send.at[src], att_recv.at[src], src, t).wait_recv()

    for copy in loads[10:14]:
        copy.wait()
    left_a = jnp.transpose(att_a[...])
    left_b = jnp.transpose(att_b[...])
    pieces = ps.shape[0]
    width = ps.shape[2]
    rs_copies = []
    for ch in range(pieces):
        at = pl.ds(ch * width, width)
        term = jnp.dot(left_a, wa[:, at], preferred_element_type=F32)
        term = term + jnp.dot(left_b, wb[:, at], preferred_element_type=F32)
        ps[ch] = term.astype(BF16)
        for j in range(1, n_tp):
            to = tp_to(j)
            copy = remote(
                ps.at[ch, pl.ds(pl.multiple_of(to * sub, sub), sub)], rs.at[ch, j - 1],
                rs_send.at[ch, j - 1], rs_recv.at[ch, j - 1], s, to,
            )
            copy.start()
            rs_copies.append(copy)
    sums = []
    for ch in range(pieces):
        at = pl.ds(ch * width, width)
        value = residual[:, at].astype(F32) + ps[
            ch, pl.ds(pl.multiple_of(t * sub, sub), sub), :
        ].astype(F32)
        for j in range(1, n_tp):
            rs_copies[ch * (n_tp - 1) + j - 1].wait_recv()
            value = value + rs[ch, j - 1].astype(F32)
        sums.append(value)
    summed = jnp.concatenate(sums, axis=1)
    center = summed - jnp.mean(summed, axis=-1, keepdims=True)
    variance = jnp.mean(center * center, axis=-1, keepdims=True)
    normed = (center * lax.rsqrt(variance + norm_eps) * gain[...]).astype(BF16)
    for i in range(n_tp):
        nb[i] = normed[:, i * feat:(i + 1) * feat]
    here = pl.ds(pl.multiple_of(t * sub, sub), sub)
    nf_copies = []
    for j in range(1, n_tp):
        to = tp_to(j)
        copy = remote(nb.at[to], nf.at[here], nf_send.at[j - 1], nf_recv.at[j - 1], s, to)
        copy.start()
        nf_copies.append(copy)
    nf[here, :] = nb[t]
    for copy in nf_copies:
        copy.wait_recv()

    spread = jnp.transpose(onehot[...].astype(F32)).astype(BF16)
    dsend[...] = jnp.dot(spread, nf[...], preferred_element_type=F32).astype(BF16).reshape(
        groups, slots, feat
    )
    d_copies = []
    for k in range(1, nz):
        zt = (z + k) % nz
        copy = remote(dsend.at[zt], xs.at[c, t, z], d_send.at[k], d_recv.at[k], 2 * zt + c, t)
        copy.start()
        d_copies.append(copy)
    xs[c, t, z] = dsend[z]
    mate = 2 * z + 1 - c
    ag_copies = []
    pair_copies = []
    for k in range(nz):
        zs = (z + nz - k) % nz
        if k:
            d_copies[k - 1].wait_recv()
        block = xs.at[c, t, zs]
        row = []
        for j in range(1, n_tp):
            copy = remote(block, block, ag_send.at[j - 1, k], ag_recv.at[j - 1, k], s, tp_to(j))
            copy.start()
            row.append(copy)
        ag_copies.append(row)
        copy = remote(block, block, pair_send.at[0, k], pair_recv.at[0, k], mate, t)
        copy.start()
        pair_copies.append([copy])

    loads[14].wait()
    loads[15].wait()
    h_copies = []
    for k in range(nz):
        zs = (z + nz - k) % nz
        for j in range(1, n_tp):
            ag_copies[k][j - 1].wait_recv()
            block = xs.at[c, tp_from(j), zs]
            copy = remote(block, block, pair_send.at[j, k], pair_recv.at[j, k], mate, t)
            copy.start()
            pair_copies[k].append(copy)
        for j in range(n_tp):
            pair_copies[k][j].wait_recv()
        rows = [
            jnp.concatenate([xs[0, i, zs], xs[1, i, zs]], axis=0) for i in range(n_tp)
        ]
        rows = jnp.concatenate(rows, axis=1)
        gate = jnp.dot(rows, gw[...], preferred_element_type=F32)
        upper = jnp.dot(rows, uw[...], preferred_element_type=F32)
        hid[zs, t] = (gate / (1.0 + jnp.exp(-gate)) * upper).astype(BF16)
        block = hid.at[zs, t]
        row = []
        for j in range(1, n_tp):
            copy = remote(block, block, h_send.at[j - 1, k], h_recv.at[j - 1, k], s, tp_to(j))
            copy.start()
            row.append(copy)
        h_copies.append(row)

    loads[16].wait()
    e_copies = []
    for k in range(nz):
        zs = (z + nz - k) % nz
        for copy in h_copies[k]:
            copy.wait_recv()
        rows = jnp.concatenate([hid[zs, i] for i in range(n_tp)], axis=1)
        result = jnp.dot(rows, dw[...], preferred_element_type=F32)
        top = result[:slots]
        bottom = result[slots:]
        own[zs] = jnp.where(c == 0, top, bottom)
        part_send[zs] = jnp.where(c == 0, bottom, top).astype(BF16)
        copy = remote(part_send.at[zs], part_got.at[zs], e_send.at[k], e_recv.at[k], mate, t)
        copy.start()
        e_copies.append(copy)

    r_copies = []
    for k in range(nz):
        zs = (z + nz - k) % nz
        if k:
            w_copies[k - 1].wait_recv()
        e_copies[k].wait_recv()
        both = wgot[zs]
        w0 = both[:, 0:1]
        w1 = both[:, 1:2]
        own_w = jnp.where(c == 0, w0, w1)
        mate_w = jnp.where(c == 0, w1, w0)
        total = (own_w * own[zs] + mate_w * part_got[zs].astype(F32)).astype(BF16)
        if k:
            ret_send[k] = total
            copy = remote(
                ret_send.at[k], ret.at[pl.ds(pl.multiple_of(z * slots, slots), slots)],
                r_send.at[k], r_recv.at[k], 2 * zs + c, t,
            )
            copy.start()
            r_copies.append(copy)
        else:
            ret[pl.ds(pl.multiple_of(z * slots, slots), slots), :] = total

    for k in range(1, nz):
        r_copies[k - 1].wait_recv()
    routed = jnp.dot(onehot[...], ret[...], preferred_element_type=F32)
    out[...] = (nf[...].astype(F32) + routed).astype(BF16)

    for core in range(2):
        @pl.when(c == core)
        def _(core=core):
            loads[9 - core].wait()
            for copy in qkv_copies(core):
                copy.wait_send()
            for dest in range(n_sp):
                @pl.when(s != dest)
                def _(dest=dest):
                    att_copy(core, dest).wait_send()
    flat = w_copies + rs_copies + nf_copies + d_copies + e_copies + r_copies
    for group in (ag_copies, pair_copies, h_copies):
        for row in group:
            flat = flat + row
    for copy in flat:
        copy.wait_send()


def fused(
    query_a, key_a, value_a, cumlog_a, query_b, key_b, value_b, cumlog_b, out_weight_a,
    out_weight_b, residual, norm_gain, expert_ids, route_weight, gate_w, up_w, down_w,
):
    n_sp = lax.axis_size("sp")
    n_tp = lax.axis_size("tp")
    nz = n_sp // 2
    tok = query_a.shape[1]
    sub = tok // n_tp
    model = residual.shape[1]
    feat = down_w.shape[2]
    inner = gate_w.shape[2]
    group_size = n_sp // GROUPS
    slots = tok // TOP
    pieces = 2
    width = model // pieces
    dims = (n_sp, n_tp, cumlog_a.shape[0], HDA, HDB, group_size)
    vmem = pl.BlockSpec(memory_space=pltpu.VMEM)
    anyw = pl.BlockSpec(memory_space=pl.ANY)
    dma = pltpu.SemaphoreType.DMA
    scratch = [
        pltpu.VMEM(query_a.shape, BF16),
        pltpu.VMEM(key_a.shape, BF16),
        pltpu.VMEM(value_a.shape, BF16),
        pltpu.VMEM(cumlog_a.shape, F32),
        pltpu.VMEM(query_b.shape, BF16),
        pltpu.VMEM(key_b.shape, BF16),
        pltpu.VMEM(value_b.shape, BF16),
        pltpu.VMEM(cumlog_b.shape, F32),
        pltpu.VMEM(residual.shape, BF16),
        pltpu.VMEM((1, model), F32),
        pltpu.VMEM((TOP, tok), jnp.int32),
        pltpu.VMEM((TOP, tok), F32),
        pltpu.VMEM(out_weight_a.shape, BF16),
        pltpu.VMEM(out_weight_b.shape, BF16),
        pltpu.VMEM(gate_w.shape[1:], BF16),
        pltpu.VMEM(up_w.shape[1:], BF16),
        pltpu.VMEM(down_w.shape[1:], BF16),
        pltpu.VMEM((3, n_sp, HDA, tok), BF16),
        pltpu.VMEM((3, n_sp, HDB, tok), BF16),
        pltpu.VMEM((n_sp * tok, tok), F32),
        pltpu.VMEM((n_sp, HDA, tok), BF16),
        pltpu.VMEM((n_sp, HDB, tok), BF16),
        pltpu.VMEM(query_a.shape, BF16),
        pltpu.VMEM(query_b.shape, BF16),
        pltpu.VMEM((pieces, tok, width), BF16),
        pltpu.VMEM((pieces, n_tp - 1, sub, width), BF16),
        pltpu.VMEM((n_tp, sub, feat), BF16),
        pltpu.VMEM((tok, feat), BF16),
        pltpu.VMEM((tok, nz * slots), BF16),
        pltpu.VMEM((nz, slots, 128), F32),
        pltpu.VMEM((nz, slots, 128), F32),
        pltpu.VMEM((nz, slots, feat), BF16),
        pltpu.VMEM((2, n_tp, nz, slots, feat), BF16),
        pltpu.VMEM((nz, n_tp, 2 * slots, inner), BF16),
        pltpu.VMEM((nz, slots, feat), F32),
        pltpu.VMEM((nz, slots, feat), BF16),
        pltpu.VMEM((nz, slots, feat), BF16),
        pltpu.VMEM((nz, slots, feat), BF16),
        pltpu.VMEM((nz * slots, feat), BF16),
        dma((17,)),
        dma((3, n_sp)), dma((3, n_sp)),
        dma((n_sp,)), dma((n_sp,)),
        dma((pieces, n_tp - 1)), dma((pieces, n_tp - 1)),
        dma((n_tp - 1,)), dma((n_tp - 1,)),
        dma((nz,)), dma((nz,)),
        dma((nz,)), dma((nz,)),
        dma((n_tp - 1, nz)), dma((n_tp - 1, nz)),
        dma((n_tp, nz)), dma((n_tp, nz)),
        dma((n_tp - 1, nz)), dma((n_tp - 1, nz)),
        dma((nz,)), dma((nz,)),
        dma((nz,)), dma((nz,)),
    ]
    return pl.pallas_call(
        functools.partial(fused_kernel, dims),
        out_shape=jax.ShapeDtypeStruct((tok, feat), BF16),
        in_specs=[anyw] * 17,
        out_specs=vmem,
        scratch_shapes=scratch,
        compiler_params=pltpu.CompilerParams(
            collective_id=0, has_side_effects=True, vmem_limit_bytes=67043328
        ),
    )(
        query_a, key_a, value_a, cumlog_a, query_b, key_b, value_b, cumlog_b, residual,
        norm_gain.reshape(1, -1), expert_ids.T, route_weight.T, out_weight_a, out_weight_b,
        gate_w, up_w, down_w,
    )


def choose(*args):
    n_sp = lax.axis_size("sp")
    heads_a = args[3].shape[0]
    heads_b = args[7].shape[0]
    fits = heads_a == heads_b and heads_a + heads_b == n_sp
    fits = fits and n_sp == GROUPS * TOP and n_sp == 2 * GROUPS
    return (fused if fits else per_device)(*args)


def solution(mesh):
    placed = (
        P("tp", "sp"),
        P("tp", "sp"),
        P("tp", "sp"),
        P("tp", None),
        P("tp", "sp"),
        P("tp", "sp"),
        P("tp", "sp"),
        P("tp", None),
        P("tp", None),
        P("tp", None),
        P(("sp", "tp"), None),
        P(),
        P("sp", None),
        P("sp", None),
        P("sp", None, "tp"),
        P("sp", None, "tp"),
        P("sp", None, "tp"),
    )
    return jax.shard_map(
        choose, mesh=mesh, in_specs=placed, out_specs=P("sp", "tp"), check_vma=False
    )
```

```python
import functools

import jax
import jax.numpy as jnp
from jax import lax
from jax.experimental import pallas as pl
from jax.experimental.pallas import tpu as pltpu
from jax.sharding import PartitionSpec as P

HDA = 64
HDB = 128
GROUPS = 4
TOP = 2


norm_eps = 1e-05


def fold_group(state, queries, keys_piece, values_piece, cum_query, cum_key, visible, head_size):
    best, total, accum = state
    heads = best.shape[0]
    count = keys_piece.shape[1]
    key_grid = keys_piece.reshape(heads, head_size, count)
    value_grid = values_piece.reshape(heads, head_size, count)
    scores = jnp.einsum(
        "hdq,hdk->hqk", queries, key_grid, preferred_element_type=jnp.float32
    ) * head_size ** (-0.5)
    scores = scores + cum_query[:, :, None] - cum_key[:, None, :]
    scores = jnp.where(visible, scores, -jnp.inf)
    best_new = jnp.max(scores, axis=-1)
    shift = jnp.where(best_new > -jnp.inf, best_new, 0.0)
    keep_old = jnp.exp(best - shift)
    weights = jnp.exp(scores - shift[:, :, None])
    total_new = total * keep_old + jnp.sum(weights, axis=-1)
    added = jnp.einsum(
        "hqk,hdk->hdq", weights.astype(jnp.bfloat16), value_grid, preferred_element_type=jnp.float32
    )
    return (best_new, total_new, accum * keep_old[:, None, :] + added)


def empty_state(heads, head_size, length):
    return (
        jnp.full((heads, length), -jnp.inf, jnp.float32),
        jnp.zeros((heads, length), jnp.float32),
        jnp.zeros((heads, head_size, length), jnp.float32),
    )


def finish_state(state):
    accum = state[2] / state[1][:, None, :]
    return accum.astype(jnp.bfloat16).reshape(-1, accum.shape[2])


def per_device(
    query_a,
    key_a,
    value_a,
    cumlog_a,
    query_b,
    key_b,
    value_b,
    cumlog_b,
    out_weight_a,
    out_weight_b,
    residual,
    norm_gain,
    expert_ids,
    route_weight,
    gate_w,
    up_w,
    down_w,
):
    local_tokens = query_a.shape[1]
    heads_a = cumlog_a.shape[0]
    heads_b = cumlog_b.shape[0]
    my_start = lax.axis_index("sp") * local_tokens
    last_query = my_start + local_tokens - 1
    query_pos = my_start + jnp.arange(local_tokens, dtype=jnp.int32)
    cum_query_a = lax.dynamic_slice_in_dim(cumlog_a, my_start, local_tokens, 1)
    cum_query_b = lax.dynamic_slice_in_dim(cumlog_b, my_start, local_tokens, 1)
    grid_a = query_a.reshape(heads_a, HDA, local_tokens)
    grid_b = query_b.reshape(heads_b, HDB, local_tokens)
    keys_a = lax.all_gather(key_a, "sp", axis=1, tiled=True)
    vals_a = lax.all_gather(value_a, "sp", axis=1, tiled=True)
    keys_b = lax.all_gather(key_b, "sp", axis=1, tiled=True)
    vals_b = lax.all_gather(value_b, "sp", axis=1, tiled=True)
    count = keys_a.shape[1]

    def visit(state):
        key_pos = jnp.arange(count, dtype=jnp.int32)
        visible = key_pos[None, None, :] <= query_pos[None, :, None]
        new_a = fold_group(state[0], grid_a, keys_a, vals_a, cum_query_a, cumlog_a, visible, HDA)
        new_b = fold_group(state[1], grid_b, keys_b, vals_b, cum_query_b, cumlog_b, visible, HDB)
        return (new_a, new_b)

    def leave(state):
        return state

    state_a, state_b = lax.cond(
        jnp.int32(0) <= last_query,
        visit,
        leave,
        (empty_state(heads_a, HDA, local_tokens), empty_state(heads_b, HDB, local_tokens)),
    )
    attn_a = finish_state(state_a)
    attn_b = finish_state(state_b)
    term = lax.dot_general(
        attn_a, out_weight_a, (((0,), (0,)), ((), ())), preferred_element_type=jnp.float32
    )
    mixed = lax.psum_scatter(
        (
            term
            + lax.dot_general(
                attn_b, out_weight_b, (((0,), (0,)), ((), ())), preferred_element_type=jnp.float32
            )
        ).astype(jnp.bfloat16),
        "tp",
        scatter_dimension=0,
        tiled=True,
    ).astype(jnp.float32)
    summed = residual.astype(jnp.float32) + mixed
    center = summed - jnp.mean(summed, axis=-1, keepdims=True)
    variance = jnp.mean(center * center, axis=-1, keepdims=True)
    normed = (center * lax.rsqrt(variance + norm_eps) * norm_gain).astype(jnp.bfloat16)
    normed_all = lax.all_gather(normed, "tp", axis=0, tiled=True)
    experts = lax.axis_size("sp")
    group_size = experts // GROUPS
    capacity = local_tokens // group_size
    features = normed_all.shape[1]
    flat_ids = expert_ids.reshape(-1)
    marks = (flat_ids[:, None] == jnp.arange(experts, dtype=jnp.int32)[None, :]).astype(jnp.int32)
    rank = jnp.sum((jnp.cumsum(marks, axis=0) - marks) * marks, axis=1)
    slot = flat_ids * capacity + rank
    token_of = jnp.arange(local_tokens * TOP, dtype=jnp.int32) // TOP
    table = jnp.zeros((experts * capacity,), jnp.int32).at[slot].set(token_of)
    filled = jnp.zeros((experts * capacity,), jnp.bfloat16).at[slot].set(1.0)
    send = (normed_all[table] * filled[:, None]).reshape(experts, capacity, features)
    rows = lax.all_to_all(send, "sp", split_axis=0, concat_axis=0, tiled=True)
    sources, items, row_width = rows.shape
    flat_rows = rows.reshape(sources * items, row_width)
    gate = jnp.dot(flat_rows, gate_w[0], preferred_element_type=jnp.float32)
    upper = jnp.dot(flat_rows, up_w[0], preferred_element_type=jnp.float32)
    hidden = (jax.nn.silu(gate) * upper).astype(jnp.bfloat16).reshape(sources, items, -1)
    hidden_all = lax.all_gather(hidden, "tp", axis=2, tiled=True)
    result = jnp.dot(
        hidden_all.reshape(sources * items, -1), down_w[0], preferred_element_type=jnp.float32
    )
    result = result.astype(jnp.bfloat16).reshape(sources, items, -1)
    returned = lax.all_to_all(result, "sp", split_axis=0, concat_axis=0, tiled=True)
    flat_back = returned.reshape(experts * capacity, -1)
    picked = flat_back[slot].reshape(local_tokens, TOP, -1).astype(jnp.float32)
    routed = jnp.sum(picked * route_weight[:, :, None], axis=1)
    columns = routed.shape[1]
    own_cols = lax.dynamic_slice_in_dim(normed_all, lax.axis_index("tp") * columns, columns, 1)
    return (own_cols.astype(jnp.float32) + routed).astype(jnp.bfloat16)


MESH = pl.DeviceIdType.MESH
F32 = jnp.float32
BF16 = jnp.bfloat16


def fused_kernel(
    dims,
    q_a_hbm, k_a_hbm, v_a_hbm, cum_a_hbm, q_b_hbm, k_b_hbm, v_b_hbm, cum_b_hbm,
    residual_hbm, gain_hbm, ids_hbm, route_hbm,
    wa_hbm, wb_hbm, gate_hbm, up_hbm, down_hbm,
    out,
    pack_a, cum_a, pack_b, cum_b, residual, gain, ids, route,
    wa, wb, gw, uw, dw,
    got_a, got_b, cols, mine_a, mine_b, att_a, att_b,
    ps, rs, nb, nf, onehot, wsend, wgot, dsend, xs, hid, own, part_send, part_got, ret_send, ret,
    w_sem, qkv_send, qkv_recv, att_send, att_recv, rs_send, rs_recv, nf_send, nf_recv,
    ws_send, ws_recv, d_send, d_recv, ag_send, ag_recv, pair_send, pair_recv,
    h_send, h_recv, e_send, e_recv, r_send, r_recv,
):
    n_sp, n_tp, heads_a, da, db, group_size = dims
    s = lax.axis_index("sp")
    t = lax.axis_index("tp")
    z = s // 2
    c = s % 2
    nz = n_sp // 2
    tok = pack_a.shape[3]
    groups = nz
    slots = dsend.shape[1]
    sub = tok // n_tp
    feat = nf.shape[1]

    def tp_to(j):
        return (t + 1 - 2 * (t % 2), (t + 2) % 4, 3 - t)[j - 1]

    def remote(src, dst, send, recv, sp, tp):
        return pltpu.make_async_remote_copy(
            src_ref=src, dst_ref=dst, send_sem=send, recv_sem=recv,
            device_id={"sp": sp, "tp": tp}, device_id_type=MESH,
        )

    loads = []
    for i, (src, dst) in enumerate(
        (
            (q_a_hbm, pack_a.at[:, 0]), (k_a_hbm, pack_a.at[:, 1]), (v_a_hbm, pack_a.at[:, 2]),
            (q_b_hbm, pack_b.at[:, 0]), (k_b_hbm, pack_b.at[:, 1]), (v_b_hbm, pack_b.at[:, 2]),
            (ids_hbm, ids), (route_hbm, route), (cum_a_hbm, cum_a), (cum_b_hbm, cum_b),
            (wa_hbm, wa), (wb_hbm, wb), (residual_hbm, residual), (gain_hbm, gain),
            (gate_hbm.at[0], gw), (up_hbm.at[0], uw), (down_hbm.at[0], dw),
        )
    ):
        copy = pltpu.make_async_copy(src, dst, w_sem.at[i])
        copy.start()
        loads.append(copy)

    barrier = pltpu.get_barrier_semaphore()
    for k in range(1, n_sp):
        pl.semaphore_signal(
            barrier, inc=1, device_id={"sp": (s + k) % n_sp, "tp": t}, device_id_type=MESH
        )
    for j in range(1, n_tp):
        pl.semaphore_signal(
            barrier, inc=1, device_id={"sp": s, "tp": tp_to(j)}, device_id_type=MESH
        )
    pl.semaphore_wait(barrier, n_sp - 1 + n_tp - 1)

    for copy in loads[:6]:
        copy.wait()
    packs = (pack_a, pack_b)
    got = (got_a, got_b)
    sizes = (da, db)

    def qkv_copies(core):
        copies = []
        for k in range(1, n_sp):
            target = (s + k) % n_sp
            kind = (core + k) % 2
            copies.append(remote(
                packs[kind].at[target // 2], got[kind].at[s], qkv_send.at[k], qkv_recv.at[s], target, t
            ))
        return copies

    for core in range(2):
        @pl.when(c == core)
        def _(core=core):
            for copy in qkv_copies(core):
                copy.start()
            got[core][s] = packs[core][z]

    loads[6].wait()
    loads[7].wait()

    def upright(row):
        return jnp.transpose(jnp.broadcast_to(row, (128, tok)))

    id0 = upright(ids[0:1, :].astype(F32))
    lane = lax.broadcasted_iota(jnp.int32, (tok, 128), 1).astype(F32)
    first = lane * group_size
    member = (id0 >= first) & (id0 < first + group_size) & (lane < groups)
    member = jnp.where(member, 1.0, 0.0)
    low = lax.broadcasted_iota(jnp.int32, (tok, tok), 1) < lax.broadcasted_iota(jnp.int32, (tok, tok), 0)
    rank = jnp.dot(
        jnp.where(low, 1.0, 0.0).astype(BF16), member.astype(BF16), preferred_element_type=F32
    )
    slot = jnp.sum(member * (rank + lane * slots), axis=1, keepdims=True)
    base = jnp.sum(member * first, axis=1, keepdims=True)
    wide = lax.broadcasted_iota(jnp.int32, (tok, groups * slots), 1).astype(F32)
    pick = jnp.where(wide == slot, 1.0, 0.0)
    onehot[...] = pick.astype(BF16)
    spread = jnp.transpose(pick).astype(BF16)
    even = id0 == base
    r0 = upright(route[0:1, :])
    r1 = upright(route[1:2, :])
    w_even = jnp.where(even, r0, r1)
    w_odd = jnp.where(even, r1, r0)
    w_lanes = jnp.where(lane == 0.0, w_even, jnp.where(lane == 1.0, w_odd, 0.0))
    hi = w_lanes.astype(BF16)
    rest = w_lanes - hi.astype(F32)
    mid = rest.astype(BF16)
    tail = (rest - mid.astype(F32)).astype(BF16)
    w_slots = (
        jnp.dot(spread, hi, preferred_element_type=F32)
        + jnp.dot(spread, mid, preferred_element_type=F32)
        + jnp.dot(spread, tail, preferred_element_type=F32)
    )
    wsend[...] = w_slots.reshape(groups, slots, 128)
    wgot[z] = wsend[z]
    w_copies = []
    for k in range(1, nz):
        zt = (z + k) % nz
        copy = remote(wsend.at[zt], wgot.at[z], ws_send.at[k], ws_recv.at[k], 2 * zt + c, t)
        copy.start()
        w_copies.append(copy)

    span = 2 * tok
    mine = (mine_a, mine_b)
    att = (att_a, att_b)
    cums = (cum_a, cum_b)

    def att_copy(core, dest):
        d = sizes[core]
        rows = pl.ds(pl.multiple_of(z * d, d), d)
        return remote(
            mine[core].at[dest], att[core].at[rows], att_send.at[dest], att_recv.at[s], dest, t
        )

    def attend(core):
        d = sizes[core]
        ref = got[core]
        loads[8 + core].wait()
        row = cums[core][pl.ds(z, 1), :]
        for j in range(n_sp):
            part = row[:, j * tok:(j + 1) * tok]
            cols[pl.ds(j * tok, tok), :] = jnp.transpose(jnp.broadcast_to(part, (tok, tok)))
        scale = d ** (-0.5)
        keys_t = []
        values = []
        for step in range(n_sp // 2):
            for src in (2 * step, 2 * step + 1):
                @pl.when(s != src)
                def _(src=src):
                    remote(
                        ref.at[src], ref.at[src], qkv_send.at[0], qkv_recv.at[src], src, t
                    ).wait_recv()
            for src in (2 * step, 2 * step + 1):
                keys_t.append(jnp.transpose(ref[src, 1]))
                values.append(ref[src, 2])
            queries = jnp.concatenate([ref[2 * step, 0], ref[2 * step + 1, 0]], axis=1)
            count = span * (step + 1)
            keys = jnp.concatenate(keys_t, axis=0)
            vals = jnp.concatenate(values, axis=1)
            score = jnp.dot(keys, queries, preferred_element_type=F32) * scale
            cum_k = cols[pl.ds(0, count), :]
            cum_q = row[:, step * span:(step + 1) * span]
            score = score + (cum_q - jnp.concatenate([cum_k, cum_k], axis=1))
            k_at = lax.broadcasted_iota(jnp.int32, (count, span), 0)
            q_at = lax.broadcasted_iota(jnp.int32, (count, span), 1) + step * span
            score = jnp.where(k_at <= q_at, score, -jnp.inf)
            best = jnp.max(score, axis=0, keepdims=True)
            weight = jnp.exp(score - best)
            total = jnp.sum(weight, axis=0, keepdims=True)
            res = jnp.dot(vals, weight.astype(BF16), preferred_element_type=F32) / total
            res = res.astype(BF16)
            for half in range(2):
                dest = 2 * step + half
                mine[core][dest] = res[:, half * tok:(half + 1) * tok]

                @pl.when(s != dest)
                def _(dest=dest):
                    att_copy(core, dest).start()

                @pl.when(s == dest)
                def _(dest=dest):
                    att[core][pl.ds(pl.multiple_of(z * d, d), d), :] = mine[core][dest]

    for core in range(2):
        @pl.when(c == core)
        def _(core=core):
            attend(core)

    for src in range(n_sp):
        core = src % 2
        d = sizes[core]

        @pl.when(s != src)
        def _(src=src, core=core, d=d):
            part = att[core].at[pl.ds((src // 2) * d, d)]
            remote(part, part, att_send.at[src], att_recv.at[src], src, t).wait_recv()

    for copy in loads[10:14]:
        copy.wait()
    left_a = jnp.transpose(att_a[...])
    left_b = jnp.transpose(att_b[...])
    pieces = ps.shape[0]
    width = ps.shape[2]
    rs_copies = []
    for ch in range(pieces):
        at = pl.ds(ch * width, width)
        term = jnp.dot(left_a, wa[:, at], preferred_element_type=F32)
        term = term + jnp.dot(left_b, wb[:, at], preferred_element_type=F32)
        ps[ch] = term.astype(BF16)
        for j in range(1, n_tp):
            to = tp_to(j)
            copy = remote(
                ps.at[ch, pl.ds(pl.multiple_of(to * sub, sub), sub)], rs.at[ch, j - 1],
                rs_send.at[ch, j - 1], rs_recv.at[ch, j - 1], s, to,
            )
            copy.start()
            rs_copies.append(copy)
    sums = []
    for ch in range(pieces):
        at = pl.ds(ch * width, width)
        value = residual[:, at].astype(F32) + ps[
            ch, pl.ds(pl.multiple_of(t * sub, sub), sub), :
        ].astype(F32)
        for j in range(1, n_tp):
            rs_copies[ch * (n_tp - 1) + j - 1].wait_recv()
            value = value + rs[ch, j - 1].astype(F32)
        sums.append(value)
    summed = jnp.concatenate(sums, axis=1)
    center = summed - jnp.mean(summed, axis=-1, keepdims=True)
    variance = jnp.mean(center * center, axis=-1, keepdims=True)
    normed = (center * lax.rsqrt(variance + norm_eps) * gain[...]).astype(BF16)
    for i in range(n_tp):
        nb[i] = normed[:, i * feat:(i + 1) * feat]
    here = pl.ds(pl.multiple_of(t * sub, sub), sub)
    nf_copies = []
    for j in range(1, n_tp):
        to = tp_to(j)
        copy = remote(nb.at[to], nf.at[here], nf_send.at[j - 1], nf_recv.at[j - 1], s, to)
        copy.start()
        nf_copies.append(copy)
    nf[here, :] = nb[t]
    for copy in nf_copies:
        copy.wait_recv()

    spread = jnp.transpose(onehot[...].astype(F32)).astype(BF16)
    dsend[...] = jnp.dot(spread, nf[...], preferred_element_type=F32).astype(BF16).reshape(
        groups, slots, feat
    )
    d_copies = []
    for k in range(1, nz):
        zt = (z + k) % nz
        copy = remote(dsend.at[zt], xs.at[c, t, z], d_send.at[k], d_recv.at[k], 2 * zt + c, t)
        copy.start()
        d_copies.append(copy)
    xs[c, t, z] = dsend[z]
    mate = 2 * z + 1 - c
    near = [t, tp_to(1), tp_to(2), tp_to(3)]
    half = slots // 2
    ag_copies = [[] for _ in range(nz)]
    pair_copies = [[] for _ in range(nz)]
    h_copies = [[] for _ in range(nz)]
    e_copies = []
    r_copies = []

    def source_chip(k):
        return (z + nz - k) % nz

    def to_pair(k, j):
        block = xs.at[c, near[j], source_chip(k)]
        copy = remote(block, block, pair_send.at[j, k], pair_recv.at[j, k], mate, t)
        copy.start()
        pair_copies[k].append(copy)

    def to_near(ref, j, sends, recvs, k, i, copies):
        copy = remote(ref, ref, sends.at[i, k], recvs.at[i, k], s, near[j])
        copy.start()
        copies[k].append(copy)

    def tokens_out(k):
        if k:
            d_copies[k - 1].wait_recv()
        block = xs.at[c, t, source_chip(k)]
        to_near(block, 1, ag_send, ag_recv, k, 0, ag_copies)
        to_near(block, 2, ag_send, ag_recv, k, 1, ag_copies)
        to_pair(k, 0)

    def tokens_relay(k):
        zs = source_chip(k)
        ag_copies[k][0].wait_recv()
        to_near(xs.at[c, near[1], zs, pl.ds(0, half)], 2, ag_send, ag_recv, k, 2, ag_copies)
        to_pair(k, 1)
        ag_copies[k][1].wait_recv()
        to_near(xs.at[c, near[2], zs, pl.ds(half, half)], 1, ag_send, ag_recv, k, 3, ag_copies)
        to_pair(k, 2)

    def hidden_out(k):
        zs = source_chip(k)
        ag_copies[k][2].wait_recv()
        ag_copies[k][3].wait_recv()
        to_pair(k, 3)
        if k == 0:
            loads[14].wait()
            loads[15].wait()
        for j in range(n_tp):
            pair_copies[k][j].wait_recv()
        rows = [
            jnp.concatenate([xs[0, i, zs], xs[1, i, zs]], axis=0) for i in range(n_tp)
        ]
        rows = jnp.concatenate(rows, axis=1)
        gate = jnp.dot(rows, gw[...], preferred_element_type=F32)
        upper = jnp.dot(rows, uw[...], preferred_element_type=F32)
        hid[zs, t] = (gate / (1.0 + jnp.exp(-gate)) * upper).astype(BF16)
        block = hid.at[zs, t]
        to_near(block, 1, h_send, h_recv, k, 0, h_copies)
        to_near(block, 2, h_send, h_recv, k, 1, h_copies)

    def hidden_relay(k):
        zs = source_chip(k)
        h_copies[k][0].wait_recv()
        to_near(hid.at[zs, near[1], pl.ds(0, slots)], 2, h_send, h_recv, k, 2, h_copies)
        h_copies[k][1].wait_recv()
        to_near(hid.at[zs, near[2], pl.ds(slots, slots)], 1, h_send, h_recv, k, 3, h_copies)

    def down(k):
        zs = source_chip(k)
        h_copies[k][2].wait_recv()
        h_copies[k][3].wait_recv()
        if k == 0:
            loads[16].wait()
        rows = jnp.concatenate([hid[zs, i] for i in range(n_tp)], axis=1)
        result = jnp.dot(rows, dw[...], preferred_element_type=F32)
        top = result[:slots]
        bottom = result[slots:]
        own[zs] = jnp.where(c == 0, top, bottom)
        part_send[zs] = jnp.where(c == 0, bottom, top).astype(BF16)
        copy = remote(part_send.at[zs], part_got.at[zs], e_send.at[k], e_recv.at[k], mate, t)
        copy.start()
        e_copies.append(copy)

    def give_back(k):
        zs = source_chip(k)
        if k:
            w_copies[k - 1].wait_recv()
        e_copies[k].wait_recv()
        both = wgot[zs]
        w0 = both[:, 0:1]
        w1 = both[:, 1:2]
        own_w = jnp.where(c == 0, w0, w1)
        mate_w = jnp.where(c == 0, w1, w0)
        total = (own_w * own[zs] + mate_w * part_got[zs].astype(F32)).astype(BF16)
        here_rows = pl.ds(pl.multiple_of(z * slots, slots), slots)
        if k:
            ret_send[k] = total
            copy = remote(
                ret_send.at[k], ret.at[here_rows], r_send.at[k], r_recv.at[k], 2 * zs + c, t
            )
            copy.start()
            r_copies.append(copy)
        else:
            ret[here_rows, :] = total

    for i in range(nz + 3):
        for stage, lag in (
            (tokens_out, 0), (tokens_relay, 1), (hidden_relay, 2), (hidden_out, 1), (down, 2),
            (give_back, 3),
        ):
            if 0 <= i - lag < nz:
                stage(i - lag)

    for k in range(1, nz):
        r_copies[k - 1].wait_recv()
    routed = jnp.dot(onehot[...], ret[...], preferred_element_type=F32)
    out[...] = (nf[...].astype(F32) + routed).astype(BF16)

    for core in range(2):
        @pl.when(c == core)
        def _(core=core):
            loads[9 - core].wait()
            for copy in qkv_copies(core):
                copy.wait_send()
            for dest in range(n_sp):
                @pl.when(s != dest)
                def _(dest=dest):
                    att_copy(core, dest).wait_send()
    flat = w_copies + rs_copies + nf_copies + d_copies + e_copies + r_copies
    for group in (ag_copies, pair_copies, h_copies):
        for row in group:
            flat = flat + row
    for copy in flat:
        copy.wait_send()


def fused(
    query_a, key_a, value_a, cumlog_a, query_b, key_b, value_b, cumlog_b, out_weight_a,
    out_weight_b, residual, norm_gain, expert_ids, route_weight, gate_w, up_w, down_w,
):
    n_sp = lax.axis_size("sp")
    n_tp = lax.axis_size("tp")
    nz = n_sp // 2
    tok = query_a.shape[1]
    sub = tok // n_tp
    model = residual.shape[1]
    feat = down_w.shape[2]
    inner = gate_w.shape[2]
    group_size = n_sp // GROUPS
    slots = tok // TOP
    pieces = 2
    width = model // pieces
    heads = cumlog_a.shape[0]
    grid_a = (heads, HDA, tok)
    grid_b = (heads, HDB, tok)
    dims = (n_sp, n_tp, heads, HDA, HDB, group_size)
    vmem = pl.BlockSpec(memory_space=pltpu.VMEM)
    anyw = pl.BlockSpec(memory_space=pl.ANY)
    dma = pltpu.SemaphoreType.DMA
    scratch = [
        pltpu.VMEM((heads, 3, HDA, tok), BF16),
        pltpu.VMEM(cumlog_a.shape, F32),
        pltpu.VMEM((heads, 3, HDB, tok), BF16),
        pltpu.VMEM(cumlog_b.shape, F32),
        pltpu.VMEM(residual.shape, BF16),
        pltpu.VMEM((1, model), F32),
        pltpu.VMEM((TOP, tok), jnp.int32),
        pltpu.VMEM((TOP, tok), F32),
        pltpu.VMEM(out_weight_a.shape, BF16),
        pltpu.VMEM(out_weight_b.shape, BF16),
        pltpu.VMEM(gate_w.shape[1:], BF16),
        pltpu.VMEM(up_w.shape[1:], BF16),
        pltpu.VMEM(down_w.shape[1:], BF16),
        pltpu.VMEM((n_sp, 3, HDA, tok), BF16),
        pltpu.VMEM((n_sp, 3, HDB, tok), BF16),
        pltpu.VMEM((n_sp * tok, tok), F32),
        pltpu.VMEM((n_sp, HDA, tok), BF16),
        pltpu.VMEM((n_sp, HDB, tok), BF16),
        pltpu.VMEM(query_a.shape, BF16),
        pltpu.VMEM(query_b.shape, BF16),
        pltpu.VMEM((pieces, tok, width), BF16),
        pltpu.VMEM((pieces, n_tp - 1, sub, width), BF16),
        pltpu.VMEM((n_tp, sub, feat), BF16),
        pltpu.VMEM((tok, feat), BF16),
        pltpu.VMEM((tok, nz * slots), BF16),
        pltpu.VMEM((nz, slots, 128), F32),
        pltpu.VMEM((nz, slots, 128), F32),
        pltpu.VMEM((nz, slots, feat), BF16),
        pltpu.VMEM((2, n_tp, nz, slots, feat), BF16),
        pltpu.VMEM((nz, n_tp, 2 * slots, inner), BF16),
        pltpu.VMEM((nz, slots, feat), F32),
        pltpu.VMEM((nz, slots, feat), BF16),
        pltpu.VMEM((nz, slots, feat), BF16),
        pltpu.VMEM((nz, slots, feat), BF16),
        pltpu.VMEM((nz * slots, feat), BF16),
        dma((17,)),
        dma((n_sp,)), dma((n_sp,)),
        dma((n_sp,)), dma((n_sp,)),
        dma((pieces, n_tp - 1)), dma((pieces, n_tp - 1)),
        dma((n_tp - 1,)), dma((n_tp - 1,)),
        dma((nz,)), dma((nz,)),
        dma((nz,)), dma((nz,)),
        dma((4, nz)), dma((4, nz)),
        dma((n_tp, nz)), dma((n_tp, nz)),
        dma((4, nz)), dma((4, nz)),
        dma((nz,)), dma((nz,)),
        dma((nz,)), dma((nz,)),
    ]
    return pl.pallas_call(
        functools.partial(fused_kernel, dims),
        out_shape=jax.ShapeDtypeStruct((tok, feat), BF16),
        in_specs=[anyw] * 17,
        out_specs=vmem,
        scratch_shapes=scratch,
        compiler_params=pltpu.CompilerParams(
            collective_id=0, has_side_effects=True, vmem_limit_bytes=67043328
        ),
    )(
        query_a.reshape(grid_a), key_a.reshape(grid_a), value_a.reshape(grid_a), cumlog_a,
        query_b.reshape(grid_b), key_b.reshape(grid_b), value_b.reshape(grid_b), cumlog_b, residual,
        norm_gain.reshape(1, -1), expert_ids.T, route_weight.T, out_weight_a, out_weight_b,
        gate_w, up_w, down_w,
    )


def choose(*args):
    n_sp = lax.axis_size("sp")
    heads_a = args[3].shape[0]
    heads_b = args[7].shape[0]
    fits = heads_a == heads_b and heads_a + heads_b == n_sp
    fits = fits and lax.axis_size("tp") == 4 and n_sp == GROUPS * TOP and n_sp == 2 * GROUPS
    return (fused if fits else per_device)(*args)


def solution(mesh):
    placed = (
        P("tp", "sp"),
        P("tp", "sp"),
        P("tp", "sp"),
        P("tp", None),
        P("tp", "sp"),
        P("tp", "sp"),
        P("tp", "sp"),
        P("tp", None),
        P("tp", None),
        P("tp", None),
        P(("sp", "tp"), None),
        P(),
        P("sp", None),
        P("sp", None),
        P("sp", None, "tp"),
        P("sp", None, "tp"),
        P("sp", None, "tp"),
    )
    return jax.shard_map(
        choose, mesh=mesh, in_specs=placed, out_specs=P("sp", "tp"), check_vma=False
    )
```

```python
import functools

import jax
import jax.numpy as jnp
from jax import lax
from jax.experimental import pallas as pl
from jax.experimental.pallas import tpu as pltpu
from jax.sharding import PartitionSpec as P

HDA = 64
HDB = 128
GROUPS = 4
TOP = 2


norm_eps = 1e-05


def fold_group(state, queries, keys_piece, values_piece, cum_query, cum_key, visible, head_size):
    best, total, accum = state
    heads = best.shape[0]
    count = keys_piece.shape[1]
    key_grid = keys_piece.reshape(heads, head_size, count)
    value_grid = values_piece.reshape(heads, head_size, count)
    scores = jnp.einsum(
        "hdq,hdk->hqk", queries, key_grid, preferred_element_type=jnp.float32
    ) * head_size ** (-0.5)
    scores = scores + cum_query[:, :, None] - cum_key[:, None, :]
    scores = jnp.where(visible, scores, -jnp.inf)
    best_new = jnp.max(scores, axis=-1)
    shift = jnp.where(best_new > -jnp.inf, best_new, 0.0)
    keep_old = jnp.exp(best - shift)
    weights = jnp.exp(scores - shift[:, :, None])
    total_new = total * keep_old + jnp.sum(weights, axis=-1)
    added = jnp.einsum(
        "hqk,hdk->hdq", weights.astype(jnp.bfloat16), value_grid, preferred_element_type=jnp.float32
    )
    return (best_new, total_new, accum * keep_old[:, None, :] + added)


def empty_state(heads, head_size, length):
    return (
        jnp.full((heads, length), -jnp.inf, jnp.float32),
        jnp.zeros((heads, length), jnp.float32),
        jnp.zeros((heads, head_size, length), jnp.float32),
    )


def finish_state(state):
    accum = state[2] / state[1][:, None, :]
    return accum.astype(jnp.bfloat16).reshape(-1, accum.shape[2])


def per_device(
    query_a,
    key_a,
    value_a,
    cumlog_a,
    query_b,
    key_b,
    value_b,
    cumlog_b,
    out_weight_a,
    out_weight_b,
    residual,
    norm_gain,
    expert_ids,
    route_weight,
    gate_w,
    up_w,
    down_w,
):
    local_tokens = query_a.shape[1]
    heads_a = cumlog_a.shape[0]
    heads_b = cumlog_b.shape[0]
    my_start = lax.axis_index("sp") * local_tokens
    last_query = my_start + local_tokens - 1
    query_pos = my_start + jnp.arange(local_tokens, dtype=jnp.int32)
    cum_query_a = lax.dynamic_slice_in_dim(cumlog_a, my_start, local_tokens, 1)
    cum_query_b = lax.dynamic_slice_in_dim(cumlog_b, my_start, local_tokens, 1)
    grid_a = query_a.reshape(heads_a, HDA, local_tokens)
    grid_b = query_b.reshape(heads_b, HDB, local_tokens)
    keys_a = lax.all_gather(key_a, "sp", axis=1, tiled=True)
    vals_a = lax.all_gather(value_a, "sp", axis=1, tiled=True)
    keys_b = lax.all_gather(key_b, "sp", axis=1, tiled=True)
    vals_b = lax.all_gather(value_b, "sp", axis=1, tiled=True)
    count = keys_a.shape[1]

    def visit(state):
        key_pos = jnp.arange(count, dtype=jnp.int32)
        visible = key_pos[None, None, :] <= query_pos[None, :, None]
        new_a = fold_group(state[0], grid_a, keys_a, vals_a, cum_query_a, cumlog_a, visible, HDA)
        new_b = fold_group(state[1], grid_b, keys_b, vals_b, cum_query_b, cumlog_b, visible, HDB)
        return (new_a, new_b)

    def leave(state):
        return state

    state_a, state_b = lax.cond(
        jnp.int32(0) <= last_query,
        visit,
        leave,
        (empty_state(heads_a, HDA, local_tokens), empty_state(heads_b, HDB, local_tokens)),
    )
    attn_a = finish_state(state_a)
    attn_b = finish_state(state_b)
    term = lax.dot_general(
        attn_a, out_weight_a, (((0,), (0,)), ((), ())), preferred_element_type=jnp.float32
    )
    mixed = lax.psum_scatter(
        (
            term
            + lax.dot_general(
                attn_b, out_weight_b, (((0,), (0,)), ((), ())), preferred_element_type=jnp.float32
            )
        ).astype(jnp.bfloat16),
        "tp",
        scatter_dimension=0,
        tiled=True,
    ).astype(jnp.float32)
    summed = residual.astype(jnp.float32) + mixed
    center = summed - jnp.mean(summed, axis=-1, keepdims=True)
    variance = jnp.mean(center * center, axis=-1, keepdims=True)
    normed = (center * lax.rsqrt(variance + norm_eps) * norm_gain).astype(jnp.bfloat16)
    normed_all = lax.all_gather(normed, "tp", axis=0, tiled=True)
    experts = lax.axis_size("sp")
    group_size = experts // GROUPS
    capacity = local_tokens // group_size
    features = normed_all.shape[1]
    flat_ids = expert_ids.reshape(-1)
    marks = (flat_ids[:, None] == jnp.arange(experts, dtype=jnp.int32)[None, :]).astype(jnp.int32)
    rank = jnp.sum((jnp.cumsum(marks, axis=0) - marks) * marks, axis=1)
    slot = flat_ids * capacity + rank
    token_of = jnp.arange(local_tokens * TOP, dtype=jnp.int32) // TOP
    table = jnp.zeros((experts * capacity,), jnp.int32).at[slot].set(token_of)
    filled = jnp.zeros((experts * capacity,), jnp.bfloat16).at[slot].set(1.0)
    send = (normed_all[table] * filled[:, None]).reshape(experts, capacity, features)
    rows = lax.all_to_all(send, "sp", split_axis=0, concat_axis=0, tiled=True)
    sources, items, row_width = rows.shape
    flat_rows = rows.reshape(sources * items, row_width)
    gate = jnp.dot(flat_rows, gate_w[0], preferred_element_type=jnp.float32)
    upper = jnp.dot(flat_rows, up_w[0], preferred_element_type=jnp.float32)
    hidden = (jax.nn.silu(gate) * upper).astype(jnp.bfloat16).reshape(sources, items, -1)
    hidden_all = lax.all_gather(hidden, "tp", axis=2, tiled=True)
    result = jnp.dot(
        hidden_all.reshape(sources * items, -1), down_w[0], preferred_element_type=jnp.float32
    )
    result = result.astype(jnp.bfloat16).reshape(sources, items, -1)
    returned = lax.all_to_all(result, "sp", split_axis=0, concat_axis=0, tiled=True)
    flat_back = returned.reshape(experts * capacity, -1)
    picked = flat_back[slot].reshape(local_tokens, TOP, -1).astype(jnp.float32)
    routed = jnp.sum(picked * route_weight[:, :, None], axis=1)
    columns = routed.shape[1]
    own_cols = lax.dynamic_slice_in_dim(normed_all, lax.axis_index("tp") * columns, columns, 1)
    return (own_cols.astype(jnp.float32) + routed).astype(jnp.bfloat16)


MESH = pl.DeviceIdType.MESH
F32 = jnp.float32
BF16 = jnp.bfloat16


def fused_kernel(
    dims,
    q_a_hbm, k_a_hbm, v_a_hbm, cum_a_hbm, q_b_hbm, k_b_hbm, v_b_hbm, cum_b_hbm,
    residual_hbm, gain_hbm, ids_hbm, route_hbm,
    wa_hbm, wb_hbm, gate_hbm, up_hbm, down_hbm,
    out,
    pack_a, cum_a, pack_b, cum_b, residual, gain, ids, route,
    wa, wb, gw, uw, dw,
    got_a, got_b, cols, mine_a, mine_b, att_a, att_b,
    ps, rs, nb, nf, onehot, wsend, wgot, dsend, xs, hid, own, part_send, part_got, ret_send, ret,
    w_sem, qkv_send, qkv_recv, att_send, att_recv, rs_send, rs_recv, nf_send, nf_recv,
    ws_send, ws_recv, d_send, d_recv, ag_send, ag_recv, pair_send, pair_recv,
    h_send, h_recv, e_send, e_recv, r_send, r_recv,
):
    n_sp, n_tp, heads_a, da, db, group_size = dims
    s = lax.axis_index("sp")
    t = lax.axis_index("tp")
    z = s // 2
    c = s % 2
    nz = n_sp // 2
    tok = pack_a.shape[3]
    groups = nz
    slots = dsend.shape[1]
    sub = tok // n_tp
    feat = nf.shape[1]

    def tp_to(j):
        return (t + 1 - 2 * (t % 2), (t + 2) % 4, 3 - t)[j - 1]

    def remote(src, dst, send, recv, sp, tp):
        return pltpu.make_async_remote_copy(
            src_ref=src, dst_ref=dst, send_sem=send, recv_sem=recv,
            device_id={"sp": sp, "tp": tp}, device_id_type=MESH,
        )

    loads = []
    for i, (src, dst) in enumerate(
        (
            (q_a_hbm, pack_a.at[:, 0]), (k_a_hbm, pack_a.at[:, 1]), (v_a_hbm, pack_a.at[:, 2]),
            (q_b_hbm, pack_b.at[:, 0]), (k_b_hbm, pack_b.at[:, 1]), (v_b_hbm, pack_b.at[:, 2]),
            (ids_hbm, ids), (route_hbm, route), (cum_a_hbm, cum_a), (cum_b_hbm, cum_b),
            (wa_hbm, wa), (wb_hbm, wb), (residual_hbm, residual), (gain_hbm, gain),
            (gate_hbm.at[0], gw), (up_hbm.at[0], uw), (down_hbm.at[0], dw),
        )
    ):
        copy = pltpu.make_async_copy(src, dst, w_sem.at[i])
        copy.start()
        loads.append(copy)

    barrier = pltpu.get_barrier_semaphore()
    for k in range(1, n_sp):
        pl.semaphore_signal(
            barrier, inc=1, device_id={"sp": (s + k) % n_sp, "tp": t}, device_id_type=MESH
        )
    for j in range(1, n_tp):
        pl.semaphore_signal(
            barrier, inc=1, device_id={"sp": s, "tp": tp_to(j)}, device_id_type=MESH
        )
    pl.semaphore_wait(barrier, n_sp - 1 + n_tp - 1)

    for copy in loads[:6]:
        copy.wait()
    packs = (pack_a, pack_b)
    got = (got_a, got_b)
    sizes = (da, db)

    def qkv_copies(core):
        copies = []
        for k in range(1, n_sp):
            target = (s + k) % n_sp
            kind = (core + k) % 2
            copies.append(remote(
                packs[kind].at[target // 2], got[kind].at[s], qkv_send.at[k], qkv_recv.at[s], target, t
            ))
        return copies

    for core in range(2):
        @pl.when(c == core)
        def _(core=core):
            for copy in qkv_copies(core):
                copy.start()
            got[core][s] = packs[core][z]

    loads[6].wait()
    loads[7].wait()

    def upright(row):
        return jnp.transpose(jnp.broadcast_to(row, (128, tok)))

    id0 = upright(ids[0:1, :].astype(F32))
    lane = lax.broadcasted_iota(jnp.int32, (tok, 128), 1).astype(F32)
    first = lane * group_size
    member = (id0 >= first) & (id0 < first + group_size) & (lane < groups)
    member = jnp.where(member, 1.0, 0.0)
    low = lax.broadcasted_iota(jnp.int32, (tok, tok), 1) < lax.broadcasted_iota(jnp.int32, (tok, tok), 0)
    rank = jnp.dot(
        jnp.where(low, 1.0, 0.0).astype(BF16), member.astype(BF16), preferred_element_type=F32
    )
    slot = jnp.sum(member * (rank + lane * slots), axis=1, keepdims=True)
    base = jnp.sum(member * first, axis=1, keepdims=True)
    wide = lax.broadcasted_iota(jnp.int32, (tok, groups * slots), 1).astype(F32)
    pick = jnp.where(wide == slot, 1.0, 0.0)
    onehot[...] = pick.astype(BF16)
    spread = jnp.transpose(pick).astype(BF16)
    even = id0 == base
    r0 = upright(route[0:1, :])
    r1 = upright(route[1:2, :])
    w_even = jnp.where(even, r0, r1)
    w_odd = jnp.where(even, r1, r0)
    w_lanes = jnp.where(lane == 0.0, w_even, jnp.where(lane == 1.0, w_odd, 0.0))
    hi = w_lanes.astype(BF16)
    rest = w_lanes - hi.astype(F32)
    mid = rest.astype(BF16)
    tail = (rest - mid.astype(F32)).astype(BF16)
    w_slots = (
        jnp.dot(spread, hi, preferred_element_type=F32)
        + jnp.dot(spread, mid, preferred_element_type=F32)
        + jnp.dot(spread, tail, preferred_element_type=F32)
    )
    wsend[...] = w_slots.reshape(groups, slots, 128)
    wgot[z] = wsend[z]
    w_copies = []
    for k in range(1, nz):
        zt = (z + k) % nz
        copy = remote(wsend.at[zt], wgot.at[z], ws_send.at[k], ws_recv.at[k], 2 * zt + c, t)
        copy.start()
        w_copies.append(copy)

    span = 2 * tok
    mine = (mine_a, mine_b)
    att = (att_a, att_b)
    cums = (cum_a, cum_b)

    def att_copy(core, dest):
        d = sizes[core]
        rows = pl.ds(pl.multiple_of(z * d, d), d)
        return remote(
            mine[core].at[dest], att[core].at[rows], att_send.at[dest], att_recv.at[s], dest, t
        )

    def attend(core):
        d = sizes[core]
        ref = got[core]
        loads[8 + core].wait()
        row = cums[core][pl.ds(z, 1), :]
        for j in range(n_sp):
            part = row[:, j * tok:(j + 1) * tok]
            cols[pl.ds(j * tok, tok), :] = jnp.transpose(jnp.broadcast_to(part, (tok, tok)))
        scale = d ** (-0.5)
        keys_t = []
        values = []
        for step in range(n_sp // 2):
            for src in (2 * step, 2 * step + 1):
                @pl.when(s != src)
                def _(src=src):
                    remote(
                        ref.at[src], ref.at[src], qkv_send.at[0], qkv_recv.at[src], src, t
                    ).wait_recv()
            for src in (2 * step, 2 * step + 1):
                keys_t.append(jnp.transpose(ref[src, 1]))
                values.append(ref[src, 2])
            queries = jnp.concatenate([ref[2 * step, 0], ref[2 * step + 1, 0]], axis=1)
            count = span * (step + 1)
            keys = jnp.concatenate(keys_t, axis=0)
            vals = jnp.concatenate(values, axis=1)
            score = jnp.dot(keys, queries, preferred_element_type=F32) * scale
            cum_k = cols[pl.ds(0, count), :]
            cum_q = row[:, step * span:(step + 1) * span]
            score = score + (cum_q - jnp.concatenate([cum_k, cum_k], axis=1))
            k_at = lax.broadcasted_iota(jnp.int32, (count, span), 0)
            q_at = lax.broadcasted_iota(jnp.int32, (count, span), 1) + step * span
            score = jnp.where(k_at <= q_at, score, -jnp.inf)
            best = jnp.max(score, axis=0, keepdims=True)
            weight = jnp.exp(score - best)
            total = jnp.sum(weight, axis=0, keepdims=True)
            res = jnp.dot(vals, weight.astype(BF16), preferred_element_type=F32) / total
            res = res.astype(BF16)
            for half in range(2):
                dest = 2 * step + half
                mine[core][dest] = res[:, half * tok:(half + 1) * tok]

                @pl.when(s != dest)
                def _(dest=dest):
                    att_copy(core, dest).start()

                @pl.when(s == dest)
                def _(dest=dest):
                    att[core][pl.ds(pl.multiple_of(z * d, d), d), :] = mine[core][dest]

    for core in range(2):
        @pl.when(c == core)
        def _(core=core):
            attend(core)

    for src in range(n_sp):
        core = src % 2
        d = sizes[core]

        @pl.when(s != src)
        def _(src=src, core=core, d=d):
            part = att[core].at[pl.ds((src // 2) * d, d)]
            remote(part, part, att_send.at[src], att_recv.at[src], src, t).wait_recv()

    for copy in loads[10:14]:
        copy.wait()
    left_a = jnp.transpose(att_a[...])
    left_b = jnp.transpose(att_b[...])
    pieces = ps.shape[0]
    width = ps.shape[2]
    rs_copies = []
    for ch in range(pieces):
        at = pl.ds(ch * width, width)
        term = jnp.dot(left_a, wa[:, at], preferred_element_type=F32)
        term = term + jnp.dot(left_b, wb[:, at], preferred_element_type=F32)
        ps[ch] = term.astype(BF16)
        for j in range(1, n_tp):
            to = tp_to(j)
            copy = remote(
                ps.at[ch, pl.ds(pl.multiple_of(to * sub, sub), sub)], rs.at[ch, j - 1],
                rs_send.at[ch, j - 1], rs_recv.at[ch, j - 1], s, to,
            )
            copy.start()
            rs_copies.append(copy)
    sums = []
    for ch in range(pieces):
        at = pl.ds(ch * width, width)
        value = residual[:, at].astype(F32) + ps[
            ch, pl.ds(pl.multiple_of(t * sub, sub), sub), :
        ].astype(F32)
        for j in range(1, n_tp):
            rs_copies[ch * (n_tp - 1) + j - 1].wait_recv()
            value = value + rs[ch, j - 1].astype(F32)
        sums.append(value)
    summed = jnp.concatenate(sums, axis=1)
    center = summed - jnp.mean(summed, axis=-1, keepdims=True)
    variance = jnp.mean(center * center, axis=-1, keepdims=True)
    normed = (center * lax.rsqrt(variance + norm_eps) * gain[...]).astype(BF16)
    for i in range(n_tp):
        nb[i] = normed[:, i * feat:(i + 1) * feat]
    here = pl.ds(pl.multiple_of(t * sub, sub), sub)
    nf_copies = []
    for j in range(1, n_tp):
        to = tp_to(j)
        copy = remote(nb.at[to], nf.at[here], nf_send.at[j - 1], nf_recv.at[j - 1], s, to)
        copy.start()
        nf_copies.append(copy)
    nf[here, :] = nb[t]
    for copy in nf_copies:
        copy.wait_recv()

    spread = jnp.transpose(onehot[...].astype(F32)).astype(BF16)
    dsend[...] = jnp.dot(spread, nf[...], preferred_element_type=F32).astype(BF16).reshape(
        groups, slots, feat
    )
    d_copies = []
    for k in range(1, nz):
        zt = (z + k) % nz
        copy = remote(dsend.at[zt], xs.at[c, t, z], d_send.at[k], d_recv.at[k], 2 * zt + c, t)
        copy.start()
        d_copies.append(copy)
    xs[c, t, z] = dsend[z]
    mate = 2 * z + 1 - c
    near = [t, tp_to(1), tp_to(2), tp_to(3)]
    ag_copies = [[] for _ in range(nz)]
    pair_copies = [[] for _ in range(nz)]
    h_copies = [[] for _ in range(nz)]
    e_copies = []
    r_copies = []

    def source_chip(k):
        return (z + nz - k) % nz

    def to_pair(k, j):
        block = xs.at[c, near[j], source_chip(k)]
        copy = remote(block, block, pair_send.at[j, k], pair_recv.at[j, k], mate, t)
        copy.start()
        pair_copies[k].append(copy)

    def to_near(ref, j, sends, recvs, k, i, copies):
        copy = remote(ref, ref, sends.at[i, k], recvs.at[i, k], s, near[j])
        copy.start()
        copies[k].append(copy)

    def tokens_out(k):
        if k:
            d_copies[k - 1].wait_recv()
        block = xs.at[c, t, source_chip(k)]
        for j in range(1, n_tp):
            to_near(block, j, ag_send, ag_recv, k, j - 1, ag_copies)
        to_pair(k, 0)

    def hidden_out(k):
        zs = source_chip(k)
        for j in range(1, n_tp):
            ag_copies[k][j - 1].wait_recv()
            to_pair(k, j)
        if k == 0:
            loads[14].wait()
            loads[15].wait()
        for j in range(n_tp):
            pair_copies[k][j].wait_recv()
        rows = [
            jnp.concatenate([xs[0, i, zs], xs[1, i, zs]], axis=0) for i in range(n_tp)
        ]
        rows = jnp.concatenate(rows, axis=1)
        gate = jnp.dot(rows, gw[...], preferred_element_type=F32)
        upper = jnp.dot(rows, uw[...], preferred_element_type=F32)
        hid[zs, t] = (gate / (1.0 + jnp.exp(-gate)) * upper).astype(BF16)
        block = hid.at[zs, t]
        for j in range(1, n_tp):
            to_near(block, j, h_send, h_recv, k, j - 1, h_copies)

    def down(k):
        zs = source_chip(k)
        for copy in h_copies[k]:
            copy.wait_recv()
        if k == 0:
            loads[16].wait()
        rows = jnp.concatenate([hid[zs, i] for i in range(n_tp)], axis=1)
        result = jnp.dot(rows, dw[...], preferred_element_type=F32)
        top = result[:slots]
        bottom = result[slots:]
        own[zs] = jnp.where(c == 0, top, bottom)
        part_send[zs] = jnp.where(c == 0, bottom, top).astype(BF16)
        copy = remote(part_send.at[zs], part_got.at[zs], e_send.at[k], e_recv.at[k], mate, t)
        copy.start()
        e_copies.append(copy)

    def give_back(k):
        zs = source_chip(k)
        if k:
            w_copies[k - 1].wait_recv()
        e_copies[k].wait_recv()
        both = wgot[zs]
        w0 = both[:, 0:1]
        w1 = both[:, 1:2]
        own_w = jnp.where(c == 0, w0, w1)
        mate_w = jnp.where(c == 0, w1, w0)
        total = (own_w * own[zs] + mate_w * part_got[zs].astype(F32)).astype(BF16)
        here_rows = pl.ds(pl.multiple_of(z * slots, slots), slots)
        if k:
            ret_send[k] = total
            copy = remote(
                ret_send.at[k], ret.at[here_rows], r_send.at[k], r_recv.at[k], 2 * zs + c, t
            )
            copy.start()
            r_copies.append(copy)
        else:
            ret[here_rows, :] = total

    for k in range(nz):
        tokens_out(k)
    for k in range(nz):
        hidden_out(k)
    for i in range(nz + 1):
        if i < nz:
            down(i)
        if i:
            give_back(i - 1)

    for k in range(1, nz):
        r_copies[k - 1].wait_recv()
    routed = jnp.dot(onehot[...], ret[...], preferred_element_type=F32)
    out[...] = (nf[...].astype(F32) + routed).astype(BF16)

    for core in range(2):
        @pl.when(c == core)
        def _(core=core):
            loads[9 - core].wait()
            for copy in qkv_copies(core):
                copy.wait_send()
            for dest in range(n_sp):
                @pl.when(s != dest)
                def _(dest=dest):
                    att_copy(core, dest).wait_send()
    flat = w_copies + rs_copies + nf_copies + d_copies + e_copies + r_copies
    for group in (ag_copies, pair_copies, h_copies):
        for row in group:
            flat = flat + row
    for copy in flat:
        copy.wait_send()


def fused(
    query_a, key_a, value_a, cumlog_a, query_b, key_b, value_b, cumlog_b, out_weight_a,
    out_weight_b, residual, norm_gain, expert_ids, route_weight, gate_w, up_w, down_w,
):
    n_sp = lax.axis_size("sp")
    n_tp = lax.axis_size("tp")
    nz = n_sp // 2
    tok = query_a.shape[1]
    sub = tok // n_tp
    model = residual.shape[1]
    feat = down_w.shape[2]
    inner = gate_w.shape[2]
    group_size = n_sp // GROUPS
    slots = tok // TOP
    pieces = 2
    width = model // pieces
    heads = cumlog_a.shape[0]
    grid_a = (heads, HDA, tok)
    grid_b = (heads, HDB, tok)
    dims = (n_sp, n_tp, heads, HDA, HDB, group_size)
    vmem = pl.BlockSpec(memory_space=pltpu.VMEM)
    anyw = pl.BlockSpec(memory_space=pl.ANY)
    dma = pltpu.SemaphoreType.DMA
    scratch = [
        pltpu.VMEM((heads, 3, HDA, tok), BF16),
        pltpu.VMEM(cumlog_a.shape, F32),
        pltpu.VMEM((heads, 3, HDB, tok), BF16),
        pltpu.VMEM(cumlog_b.shape, F32),
        pltpu.VMEM(residual.shape, BF16),
        pltpu.VMEM((1, model), F32),
        pltpu.VMEM((TOP, tok), jnp.int32),
        pltpu.VMEM((TOP, tok), F32),
        pltpu.VMEM(out_weight_a.shape, BF16),
        pltpu.VMEM(out_weight_b.shape, BF16),
        pltpu.VMEM(gate_w.shape[1:], BF16),
        pltpu.VMEM(up_w.shape[1:], BF16),
        pltpu.VMEM(down_w.shape[1:], BF16),
        pltpu.VMEM((n_sp, 3, HDA, tok), BF16),
        pltpu.VMEM((n_sp, 3, HDB, tok), BF16),
        pltpu.VMEM((n_sp * tok, tok), F32),
        pltpu.VMEM((n_sp, HDA, tok), BF16),
        pltpu.VMEM((n_sp, HDB, tok), BF16),
        pltpu.VMEM(query_a.shape, BF16),
        pltpu.VMEM(query_b.shape, BF16),
        pltpu.VMEM((pieces, tok, width), BF16),
        pltpu.VMEM((pieces, n_tp - 1, sub, width), BF16),
        pltpu.VMEM((n_tp, sub, feat), BF16),
        pltpu.VMEM((tok, feat), BF16),
        pltpu.VMEM((tok, nz * slots), BF16),
        pltpu.VMEM((nz, slots, 128), F32),
        pltpu.VMEM((nz, slots, 128), F32),
        pltpu.VMEM((nz, slots, feat), BF16),
        pltpu.VMEM((2, n_tp, nz, slots, feat), BF16),
        pltpu.VMEM((nz, n_tp, 2 * slots, inner), BF16),
        pltpu.VMEM((nz, slots, feat), F32),
        pltpu.VMEM((nz, slots, feat), BF16),
        pltpu.VMEM((nz, slots, feat), BF16),
        pltpu.VMEM((nz, slots, feat), BF16),
        pltpu.VMEM((nz * slots, feat), BF16),
        dma((17,)),
        dma((n_sp,)), dma((n_sp,)),
        dma((n_sp,)), dma((n_sp,)),
        dma((pieces, n_tp - 1)), dma((pieces, n_tp - 1)),
        dma((n_tp - 1,)), dma((n_tp - 1,)),
        dma((nz,)), dma((nz,)),
        dma((nz,)), dma((nz,)),
        dma((4, nz)), dma((4, nz)),
        dma((n_tp, nz)), dma((n_tp, nz)),
        dma((4, nz)), dma((4, nz)),
        dma((nz,)), dma((nz,)),
        dma((nz,)), dma((nz,)),
    ]
    return pl.pallas_call(
        functools.partial(fused_kernel, dims),
        out_shape=jax.ShapeDtypeStruct((tok, feat), BF16),
        in_specs=[anyw] * 17,
        out_specs=vmem,
        scratch_shapes=scratch,
        compiler_params=pltpu.CompilerParams(
            collective_id=0, has_side_effects=True, vmem_limit_bytes=67043328
        ),
    )(
        query_a.reshape(grid_a), key_a.reshape(grid_a), value_a.reshape(grid_a), cumlog_a,
        query_b.reshape(grid_b), key_b.reshape(grid_b), value_b.reshape(grid_b), cumlog_b, residual,
        norm_gain.reshape(1, -1), expert_ids.T, route_weight.T, out_weight_a, out_weight_b,
        gate_w, up_w, down_w,
    )


def choose(*args):
    n_sp = lax.axis_size("sp")
    heads_a = args[3].shape[0]
    heads_b = args[7].shape[0]
    fits = heads_a == heads_b and heads_a + heads_b == n_sp
    fits = fits and lax.axis_size("tp") == 4 and n_sp == GROUPS * TOP and n_sp == 2 * GROUPS
    return (fused if fits else per_device)(*args)


def solution(mesh):
    placed = (
        P("tp", "sp"),
        P("tp", "sp"),
        P("tp", "sp"),
        P("tp", None),
        P("tp", "sp"),
        P("tp", "sp"),
        P("tp", "sp"),
        P("tp", None),
        P("tp", None),
        P("tp", None),
        P(("sp", "tp"), None),
        P(),
        P("sp", None),
        P("sp", None),
        P("sp", None, "tp"),
        P("sp", None, "tp"),
        P("sp", None, "tp"),
    )
    return jax.shard_map(
        choose, mesh=mesh, in_specs=placed, out_specs=P("sp", "tp"), check_vma=False
    )
```
